128 devices in a mesh: rep: 16 (over z, x), fs: 4 (over y), tp: 2 (over core).
Axes of the slice: x: 4, y: 4, z: 4, core: 2. Of those that a mesh axis runs over, the one named last changes fastest.
Arguments:
- tokens_in: bfloat16 [32768, 2048], P(('rep', 'fs', 'tp')), may hold values from -6 to 6
- norm_gain: float32 [2048], replicated, may hold values from 0.1 to 1.9
- gate_weight: bfloat16 [2048, 3072], P(None, ('fs', 'tp')), may hold values from -0.125 to 0.125
- up_weight: bfloat16 [2048, 3072], P(None, ('fs', 'tp')), may hold values from -0.125 to 0.125
- down_weight: bfloat16 [3072, 2048], P(('fs', 'tp')), may hold values from -0.109375 to 0.109375
- out_grad: bfloat16 [32768, 2048], P(('rep', 'fs', 'tp')), may hold values from -24 to 24
Outputs:
- grad_in: bfloat16 [32768, 2048], P(('rep', 'fs', 'tp'))
- grad_gain: float32 [2048], replicated
- grad_gate: float32 [2048, 3072], P(None, ('fs', 'tp'))
- grad_up: float32 [2048, 3072], P(None, ('fs', 'tp'))
- grad_down: float32 [3072, 2048], P(('fs', 'tp'))
The draws below stay inside these ranges and needn't reach their ends.
All inputs are finite; a program needn't handle non-finite values.
Results may differ from the reference program's by a relative error of at most 0.014.
Values may be sent and summed in bfloat16 or wider, within the bound.
A program may use at most 192 MiB of HBM per device.

```python
import jax
import jax.numpy as jnp
from jax import lax

D = 2048
FF = 3072
TOKENS = 32768
BLOCKS = 8


def strengthened(entries, key, source, target, shards_of, factor):
    def block_of(axis_at):
        return (jnp.arange(entries.shape[axis_at]) // (entries.shape[axis_at] // shards_of)).reshape((-1,) + (1,) * (entries.ndim - 1 - axis_at))

    first = jax.random.permutation(key, shards_of)[block_of(target)]
    far = (block_of(target) + shards_of // 2) % shards_of
    return jnp.where((block_of(source) == first) | (block_of(source) == far), factor * entries, entries)


def shard_levels(rng, dims, split, smallest, high):
    factor_of, own = 1.0, jax.random.fold_in(rng, 6)
    for axis_at, shards_of in split:
        draws = jnp.exp(jax.random.uniform(jax.random.fold_in(own, axis_at), (shards_of,), jnp.float32, smallest / len(split), high / len(split)))
        factor_of = factor_of * jnp.repeat(draws, dims[axis_at] // shards_of).reshape([-1 if axis == axis_at else 1 for axis in range(len(dims))])
    return factor_of


def normal_values(rng, extent, scale, most, cuts=(), held_as=jnp.bfloat16):
    drawn = jax.random.normal(rng, extent, jnp.float32) * scale
    if len(cuts) > 0:
        drawn = shard_levels(rng, extent, cuts, -0.22, 0.18) * drawn
    return jnp.clip(drawn, min=-most, max=most).astype(held_as)


def noise_with(key, dims, scale, reach, shards, heavy, dtype=jnp.bfloat16):
    array = scale * jax.random.normal(key, dims, jnp.float32)
    if shards:
        array = array * shard_levels(key, dims, shards, -0.22, 0.18)
    return jnp.clip(strengthened(array, jax.random.fold_in(key, 3), *heavy), -reach, reach).astype(dtype)


def setup_inputs(seed: int = 0) -> dict:
    key_of = jax.random.split(jax.random.key(seed), 7)
    return {
        "tokens_in": normal_values(key_of[0], (TOKENS, D), 1.0, 6.0, ((0, 128),)),
        "norm_gain": jnp.clip(1.0 + 0.18 * jax.random.normal(key_of[1], (D,), jnp.float32), 0.1, 1.9),
        "gate_weight": normal_values(key_of[2], (D, FF), D ** -0.5, 0.125, ((1, 8),)),
        "up_weight": normal_values(key_of[3], (D, FF), D ** -0.5, 0.125, ((1, 8),)),
        "down_weight": normal_values(key_of[4], (FF, D), FF ** -0.5, 0.109375, ((0, 8),)),
        "out_grad": noise_with(key_of[5], (TOKENS, D), 1.0, 24.0, ((0, 128),), (0, 1, 128, 5.5)),
    }


norm_eps = 1e-06

def reference(tokens_in, norm_gain, gate_weight, up_weight, down_weight, out_grad):
    floats = tokens_in.astype(jnp.float32)
    inverse = lax.rsqrt(lax.optimization_barrier(jnp.mean(floats * floats, axis=-1, keepdims=True)) + norm_eps)
    unit_rows = floats * inverse
    normed = (unit_rows * norm_gain).astype(jnp.bfloat16)
    gate_pre = jnp.dot(normed, gate_weight, preferred_element_type=jnp.float32)
    up_pre = jnp.dot(normed, up_weight, preferred_element_type=jnp.float32)
    sigma = jax.nn.sigmoid(gate_pre)
    active = gate_pre * sigma
    hidden = (active * up_pre).astype(jnp.bfloat16)
    grad_hidden = 0.5 * jnp.dot(out_grad, down_weight.T, preferred_element_type=jnp.float32)
    grad_gate_pre = (grad_hidden * up_pre * sigma * (1.0 + gate_pre * (1.0 - sigma))).astype(jnp.bfloat16)
    grad_up_pre = (grad_hidden * active).astype(jnp.bfloat16)
    factor = float(TOKENS) ** (-0.5)
    grad_down = jnp.dot(hidden.T, out_grad, preferred_element_type=jnp.float32) * (0.5 * factor)
    grad_gate = jnp.dot(normed.T, grad_gate_pre, preferred_element_type=jnp.float32) * factor
    grad_up = jnp.dot(normed.T, grad_up_pre, preferred_element_type=jnp.float32) * factor
    width = FF // BLOCKS
    grad_normed = jnp.zeros(floats.shape, jnp.float32)
    for block in range(BLOCKS):
        lower = block * width
        term = jnp.dot(grad_gate_pre[:, lower:lower + width], gate_weight[:, lower:lower + width].T, preferred_element_type=jnp.float32)
        term = term + jnp.dot(grad_up_pre[:, lower:lower + width], up_weight[:, lower:lower + width].T, preferred_element_type=jnp.float32)
        grad_normed = grad_normed + term.astype(jnp.bfloat16).astype(jnp.float32)
    grad_gain = lax.optimization_barrier(jnp.sum(grad_normed * unit_rows, axis=0))
    scaled = grad_normed * norm_gain
    grad_in = out_grad.astype(jnp.float32) + inverse * scaled - unit_rows * inverse * lax.optimization_barrier(jnp.mean(scaled * unit_rows, axis=-1, keepdims=True))
    return (grad_in.astype(jnp.bfloat16), grad_gain, grad_gate, grad_up, grad_down)
```

```python
import jax
import jax.numpy as jnp
from jax import lax
from jax.experimental import pallas as pl
from jax.experimental.pallas import tpu as pltpu
from jax.sharding import PartitionSpec as P

norm_eps = 1e-06
MESH = pl.DeviceIdType.MESH
F32 = jnp.float32
BF16 = jnp.bfloat16

D = 2048
FF = 384
ROWS = 256
PIECE = 64
HALF = 128
STEPS = 8
CH = 256
UNITS = (64, 96)
WIDTHS = (2 * FF, CH)


def over(n, step, body):
    def go(i, carry):
        body(pl.multiple_of(i * step, step))
        return carry

    lax.fori_loop(0, n // step, go, 0)


def dot(a, b, ca, cb):
    return lax.dot_general(a, b, (((ca,), (cb,)), ((), ())), preferred_element_type=F32)


def kernel(
    x_in, gain_in, gate_in, up_in, down_in, g_in,
    gin_out, gain_out, gu_out, dn_out,
    xg, wgu, wdn, gain, acc_gu, acc_dn, nrm, pre, gh, dgu, hid,
    kept, away, from_sib, far_l, far_r, near_l, near_r,
    wg, wd, s1g, s1d, t1g, t1d, vg, vd, s2g, s2d, t2g, t2d, og, od,
    g_tp, g_y, g_x, g_z,
    ld_sem, ag_send, ag_recv, sib_send, sib_recv, rs_send, rs_recv,
    ar_send, ar_recv, gn_send, gn_recv,
):
    rep, fs, tp = lax.axis_index("rep"), lax.axis_index("fs"), lax.axis_index("tp")
    z, x = rep // 4, rep % 4

    def y_at(k):
        return {"rep": rep, "fs": (fs + k) % 4, "tp": tp}

    def x_at(k):
        return {"rep": z * 4 + (x + k) % 4, "fs": fs, "tp": tp}

    def z_at(k):
        return {"rep": ((z + k) % 4) * 4 + x, "fs": fs, "tp": tp}

    sib = {"rep": rep, "fs": fs, "tp": 1 - tp}

    def remote(src, dst, send, recv, to):
        return pltpu.make_async_remote_copy(
            src_ref=src, dst_ref=dst, send_sem=send, recv_sem=recv, device_id=to, device_id_type=MESH
        )

    loads = []
    for s in range(2):
        loads.append(pltpu.make_async_copy(x_in.at[pl.ds(s * HALF, HALF)], xg.at[s, 0, pl.ds(0, HALF)], ld_sem.at[2 * s]))
        loads.append(pltpu.make_async_copy(g_in.at[pl.ds(s * HALF, HALF)], xg.at[s, 1, pl.ds(0, HALF)], ld_sem.at[2 * s + 1]))
    loads.append(pltpu.make_async_copy(gate_in, wgu.at[:, pl.ds(0, FF)], ld_sem.at[4]))
    loads.append(pltpu.make_async_copy(up_in, wgu.at[:, pl.ds(FF, FF)], ld_sem.at[5]))
    loads.append(pltpu.make_async_copy(down_in, wdn, ld_sem.at[6]))
    loads.append(pltpu.make_async_copy(gain_in, gain, ld_sem.at[7]))
    for c in loads:
        c.start()

    barrier = pltpu.get_barrier_semaphore()
    partners = [sib] + [at(k) for at in (y_at, x_at, z_at) for k in (1, 3, 2)]
    for p in partners:
        pl.semaphore_signal(barrier, inc=1, device_id=p, device_id_type=MESH)
    pl.semaphore_wait(barrier, len(partners))

    def to_sib(s):
        return remote(
            xg.at[s, :, pl.ds(0, HALF)], xg.at[s, :, pl.ds(HALF, HALF)], ag_send.at[s], ag_recv.at[s, 2], sib
        )

    def own_piece(p, j):
        src = xg.at[p // 2, :, pl.ds((p % 2) * PIECE, PIECE)]
        dst = xg.at[2 + p, :, pl.ds(j * PIECE, PIECE)]
        return remote(src, dst, ag_send.at[8 + 2 * p + j], ag_recv.at[2 + p, j], y_at(1 if j == 0 else 3))

    def onward(s, j):
        return remote(
            xg.at[s, :, pl.ds(j * PIECE, PIECE)],
            xg.at[s + 4 - 2 * j, :, pl.ds(j * PIECE, PIECE)],
            ag_send.at[14 + s],
            ag_recv.at[s + 4 - 2 * j, j],
            y_at(1 if j == 0 else 3),
        )

    def arrival(s, j):
        ref = xg.at[s, :, pl.ds(j * PIECE, PIECE)]
        return remote(ref, ref, ag_send.at[0], ag_recv.at[s, j], sib)

    for s in range(2):
        loads[2 * s].wait()
        loads[2 * s + 1].wait()
        for p in (2 * s, 2 * s + 1):
            own_piece(p, 0).start()
            own_piece(p, 1).start()
        to_sib(s).start()
    for c in loads[4:]:
        c.wait()

    def zero(r):
        acc_gu[pl.ds(r, 64), :] = jnp.zeros((64, 2 * FF), F32)
        acc_dn[pl.ds(pl.multiple_of(r // 64 * 96, 96), 96), :] = jnp.zeros((96, CH), F32)

    over(D, 64, zero)

    def sib_sum(s):
        return remote(away.at[s % 2], from_sib.at[s], sib_send.at[s % 2], sib_recv.at[s], sib)

    def chip_sum(s):
        sib_sum(s).wait_recv()

        def add(r):
            rows = pl.ds(r, 32)
            kept[s, rows, :] = (kept[s, rows, :].astype(F32) + from_sib[s, rows, :].astype(F32)).astype(BF16)

        over(HALF, 32, add)

    def early_right(q):
        return remote(kept.at[q, pl.ds(PIECE, PIECE)], near_l.at[q - 2], rs_send.at[q], rs_recv.at[0, q - 2], y_at(1))

    def early_left(q):
        return remote(kept.at[q, pl.ds(0, PIECE)], near_r.at[q - 2], rs_send.at[q], rs_recv.at[1, q - 2], y_at(3))

    def far_left(q):
        return remote(kept.at[q, pl.ds(0, PIECE)], far_r.at[q - 6], rs_send.at[q], rs_recv.at[2, q - 6], y_at(3))

    def far_right(q):
        return remote(kept.at[q, pl.ds(PIECE, PIECE)], far_l.at[q - 6], rs_send.at[q + 2], rs_recv.at[2, q - 4], y_at(1))

    def late_left(q):
        return remote(kept.at[q, pl.ds(0, PIECE)], near_r.at[q - 2], rs_send.at[q + 8], rs_recv.at[1, q - 2], y_at(3))

    def late_right(q):
        return remote(kept.at[q, pl.ds(PIECE, PIECE)], near_l.at[q - 2], rs_send.at[q + 8], rs_recv.at[0, q - 2], y_at(1))

    def step(s, carry):
        @pl.when(s >= 2)
        def _():
            arrival(s, 0).wait_recv()
            arrival(s, 1).wait_recv()
            to_sib(s).start()

        @pl.when((s == 2) | (s == 3))
        def _():
            onward(s, 0).start()

        @pl.when((s == 4) | (s == 5))
        def _():
            onward(s, 1).start()

        to_sib(s).wait_recv()

        def norm(r):
            rows = pl.ds(r, 16)
            floats = xg[s, 0, rows, :].astype(F32)
            inverse = lax.rsqrt(jnp.mean(floats * floats, axis=-1, keepdims=True) + norm_eps)
            nrm[rows, :] = (floats * inverse * gain[...]).astype(BF16)

        over(ROWS, 16, norm)
        pre[...] = dot(nrm[...], wgu[...], 1, 0)
        gh[...] = dot(xg[s, 1], wdn[...], 1, 1)

        def gates(r):
            rows = pl.ds(r, 32)
            gate_pre, up_pre = pre[rows, :FF], pre[rows, FF:]
            grad_hidden = 0.5 * gh[rows, :]
            sigma = jax.nn.sigmoid(gate_pre)
            active = gate_pre * sigma
            hid[rows, :] = (active * up_pre).astype(BF16)
            dgu[rows, :FF] = (grad_hidden * up_pre * sigma * (1.0 + gate_pre * (1.0 - sigma))).astype(BF16)
            dgu[rows, FF:] = (grad_hidden * active).astype(BF16)

        over(ROWS, 32, gates)

        @pl.when(s >= 2)
        def _():
            sib_sum(s).wait_send()

        def terms(c):
            cols = pl.ds(c, CH)
            term = dot(dgu[...], wgu[cols, :], 1, 1).astype(BF16)
            kept[s, :, cols] = term[:HALF]
            away[s % 2, :, cols] = term[HALF:]

        over(D, CH, terms)

        def weights(c):
            cols = pl.ds(c, CH)
            acc_gu[cols, :] += dot(nrm[:, cols], dgu[...], 0, 0)
            rows = pl.ds(pl.multiple_of(c // CH * FF, FF), FF)
            acc_dn[rows, :] += dot(hid[...], xg[s, 1, :, cols], 0, 0)

        over(D, CH, weights)
        sib_sum(s).start()

        @pl.when(s >= 1)
        def _():
            chip_sum(s - 1)

        @pl.when((s == 3) | (s == 4))
        def _():
            early_right(s - 1).start()

        @pl.when((s == 5) | (s == 6))
        def _():
            early_left(s - 1).start()

        return carry

    lax.fori_loop(0, STEPS, step, 0)

    packed = ((wg, s1g, t1g, vg, s2g, t2g, og, gu_out), (wd, s1d, t1d, vd, s2d, t2d, od, dn_out))
    halves = ((x, z, x_at, z_at), (z, x, z_at, x_at))
    streams = [(h, k) for k in range(2) for h in range(2)]

    class Ring:
        def __init__(self, h, k, src, base, size, mid, end, index, at, sem):
            self.src, self.size, self.mid, self.end = src, size, mid, end
            half = size // 2
            self.half = half
            f = h * 2 + k

            def rows(chunk, part):
                start = base + ((index + chunk) % 4) * size + part * half
                return pl.ds(pl.multiple_of(start, 16), half)

            self.rows = rows

            def copy(i, chunk, part, dst, to):
                return remote(src.at[rows(chunk, part)], dst, ar_send.at[f, sem + i], ar_recv.at[f, sem + i], at(to))

            self.first = [
                copy(0, 2, 0, mid.at[h, 1], 3),
                copy(1, 2, 1, mid.at[h, 0], 1),
                copy(2, 3, 1, end.at[h, 1, pl.ds(half, half)], 3),
                copy(3, 1, 0, end.at[h, 0, pl.ds(0, half)], 1),
            ]
            self.second = [
                copy(4, 3, 0, end.at[h, 1, pl.ds(0, half)], 3),
                copy(5, 1, 1, end.at[h, 0, pl.ds(half, half)], 1),
            ]
            self.h = h

        def issue(self):
            for c in self.first:
                c.start()

        def relay(self):
            h = self.h
            for i, (chunk, part, side) in enumerate(((3, 0, 1), (1, 1, 0))):
                self.first[i].wait_recv()
                rows = self.rows(chunk, part)
                self.src[rows, :] = (self.src[rows, :].astype(F32) + self.mid[h, side].astype(F32)).astype(BF16)
                self.second[i].start()

        def finish(self, store):
            h = self.h
            for c in self.first[2:] + self.second:
                c.wait_recv()
            for part in range(2):
                local = pl.ds(part * self.half, self.half)
                total = self.src[self.rows(0, part), :].astype(F32)
                total = total + self.end[h, 0, local, :].astype(F32) + self.end[h, 1, local, :].astype(F32)
                store(part, total.astype(BF16))

        def drain(self):
            for c in self.first + self.second:
                c.wait_send()

    rings1, rings2 = {}, {}
    for h, k in streams:
        w, s1, t1, v, s2, t2, o, out = packed[k]
        i1, i2, at1, at2 = halves[h]
        unit = UNITS[k]
        rings1[h, k] = Ring(h, k, w, h * 16 * unit, 4 * unit, s1, t1, i1, at1, 0)
        rings2[h, k] = Ring(h, k, v, h * 4 * unit, unit, s2, t2, i2, at2, 6)

    def cast_gu(r):
        wg[pl.ds(r, 64), :] = acc_gu[pl.ds(r, 64), :].astype(BF16)

    def cast_dn(r):
        wd[pl.ds(r, 96), :] = acc_dn[pl.ds(r, 96), :].astype(BF16)

    over(D, 64, cast_gu)
    for h in range(2):
        rings1[h, 0].issue()
    over(8 * FF, 96, cast_dn)
    far_left(6).start()
    far_right(6).start()
    for h in range(2):
        rings1[h, 1].issue()
    chip_sum(7)
    far_left(7).start()
    far_right(7).start()

    for h in range(2):
        rings1[h, 0].relay()

    def add_far(q, lo, far, wait):
        wait.wait_recv()

        def add(r):
            rows = pl.ds(lo + r, 32)
            kept[q, rows, :] = (kept[q, rows, :].astype(F32) + far[pl.ds(r, 32), :].astype(F32)).astype(BF16)

        over(PIECE, 32, add)

    for i in range(2):
        add_far(2 + i, 0, far_r.at[i], far_left(6 + i))
        late_left(2 + i).start()
        add_far(4 + i, PIECE, far_l.at[i], far_right(6 + i))
        late_right(4 + i).start()
    for h in range(2):
        rings1[h, 1].relay()

    def store_v(h, k):
        v, unit = packed[k][3], UNITS[k]

        def store(part, value):
            v[pl.ds(h * 4 * unit + part * 2 * unit, 2 * unit), :] = value

        return store

    def store_o(h, k):
        o, unit = packed[k][6], UNITS[k]

        def store(part, value):
            o[h, pl.ds(part * (unit // 2), unit // 2), :] = value

        return store

    for h, k in streams:
        rings1[h, k].finish(store_v(h, k))
        rings2[h, k].issue()
    for h, k in streams:
        rings2[h, k].relay()

    class Gather:
        def __init__(self, h, k, src, base, size, index, at, sem):
            out, f, half = packed[k][7], h * 2 + k, size // 2

            def where(chunk, part=None):
                start = base + ((index + chunk) % 4) * size
                if part is None:
                    return pl.ds(pl.multiple_of(start, 16), size)
                return pl.ds(pl.multiple_of(start + part * half, 16), half)

            mine = out.at[where(0)] if src is None else src
            self.own = []
            for i, to in enumerate((1, 3)):
                self.own.append(
                    remote(mine, out.at[where(0)], ar_send.at[f, sem + i], ar_recv.at[f, sem + i], at(to))
                )
            self.near = [
                remote(out.at[where(c)], out.at[where(c)], ar_send.at[f, sem + i], ar_recv.at[f, sem + i], at(1))
                for i, c in enumerate((3, 1))
            ]
            self.on = [
                remote(out.at[where(c, i)], out.at[where(c, i)], ar_send.at[f, sem + 2 + i], ar_recv.at[f, sem + 2 + i], at(to))
                for i, (c, to) in enumerate(((3, 1), (1, 3)))
            ]
            self.far = [
                remote(out.at[where(2, i)], out.at[where(2, i)], ar_send.at[f, sem + 2 + i], ar_recv.at[f, sem + 2 + i], at(1))
                for i in range(2)
            ]

        def issue(self):
            for c in self.own:
                c.start()

        def relay(self):
            for near, on in zip(self.near, self.on):
                near.wait_recv()
                on.start()

        def finish(self):
            for c in self.far:
                c.wait_recv()

        def drain(self):
            for c in self.own + self.on:
                c.wait_send()

    back2, back1, homes = {}, {}, {}
    for h, k in streams:
        i1, i2, at1, at2 = halves[h]
        unit, o, out = UNITS[k], packed[k][6], packed[k][7]
        base = (h * 4 + i1) * 4 * unit
        back2[h, k] = Gather(h, k, o.at[h], base, unit, i2, at2, 12)
        back1[h, k] = Gather(h, k, None, h * 16 * unit, 4 * unit, i1, at1, 16)
        homes[h, k] = pltpu.make_async_copy(
            o.at[h], out.at[pl.ds(pl.multiple_of(base + i2 * unit, 16), unit)], ar_send.at[h * 2 + k, 20]
        )

    for h, k in streams:
        rings2[h, k].finish(store_o(h, k))
        homes[h, k].start()
        back2[h, k].issue()

    late_left(2).wait_recv()
    late_left(3).wait_recv()
    early_left(4).wait_recv()
    early_left(5).wait_recv()
    early_right(2).wait_recv()
    early_right(3).wait_recv()
    late_right(4).wait_recv()
    late_right(5).wait_recv()
    g_tp[tp] = jnp.zeros((8, D), F32)

    def own_rows(i, carry):
        r = pl.multiple_of(i * 16, 16)
        s, p = i // 8, i // 4
        half, piece = pl.ds(pl.multiple_of((i % 8) * 16, 16), 16), pl.ds(pl.multiple_of((i % 4) * 16, 16), 16)
        grad = kept[s, half, :].astype(F32) + near_l[p, piece, :].astype(F32) + near_r[p, piece, :].astype(F32)
        floats = xg[s, 0, half, :].astype(F32)
        inverse = lax.rsqrt(jnp.mean(floats * floats, axis=-1, keepdims=True) + norm_eps)
        unit_rows = floats * inverse
        gained = grad * unit_rows
        g_tp[tp] += gained[:8] + gained[8:]
        scaled = grad * gain[...]
        mean = jnp.mean(scaled * unit_rows, axis=-1, keepdims=True)
        result = xg[s, 1, half, :].astype(F32) + inverse * scaled - unit_rows * inverse * mean
        gin_out[pl.ds(r, 16), :] = result.astype(BF16)
        return carry

    lax.fori_loop(0, ROWS // 16, own_rows, 0)

    gains = []

    def spread(buffer, index, targets, first):
        copies = [
            remote(buffer.at[index], buffer.at[index], gn_send.at[first + i], gn_recv.at[first + i], to)
            for i, to in enumerate(targets)
        ]
        gains.extend(copies)
        for c in copies:
            c.start()
        return copies

    g1 = spread(g_tp, tp, [sib], 0)
    for h, k in streams:
        back2[h, k].relay()
    g1[0].wait_recv()
    g_y[fs] = g_tp[0] + g_tp[1]
    g2 = spread(g_y, fs, [y_at(1), y_at(2), y_at(3)], 1)
    for h, k in streams:
        back2[h, k].finish()
        homes[h, k].wait()
        back1[h, k].issue()
    for c in g2:
        c.wait_recv()
    g_x[x] = (g_y[0] + g_y[1]) + (g_y[2] + g_y[3])
    g3 = spread(g_x, x, [x_at(1), x_at(2), x_at(3)], 4)
    for c in g3:
        c.wait_recv()
    g_z[z] = (g_x[0] + g_x[1]) + (g_x[2] + g_x[3])
    g4 = spread(g_z, z, [z_at(1), z_at(2), z_at(3)], 7)
    for c in g4:
        c.wait_recv()
    gain_out[...] = (g_z[0] + g_z[1]) + (g_z[2] + g_z[3])
    for h, k in streams:
        back1[h, k].relay()
    for h, k in streams:
        back1[h, k].finish()

    for s in range(STEPS):
        to_sib(s).wait_send()
    for p in range(4):
        own_piece(p, 0).wait_send()
        own_piece(p, 1).wait_send()
    for s in range(2, 6):
        onward(s, 0 if s < 4 else 1).wait_send()
    sib_sum(6).wait_send()
    sib_sum(7).wait_send()
    for q in (2, 3):
        early_right(q).wait_send()
        late_left(q).wait_send()
    for q in (4, 5):
        early_left(q).wait_send()
        late_right(q).wait_send()
    for q in (6, 7):
        far_left(q).wait_send()
        far_right(q).wait_send()
    for h, k in streams:
        rings1[h, k].drain()
        rings2[h, k].drain()
        back2[h, k].drain()
        back1[h, k].drain()
    for c in gains:
        c.wait_send()


def fused(tokens_in, norm_gain, gate_weight, up_weight, down_weight, out_grad):
    any_space = pl.BlockSpec(memory_space=pl.ANY)
    vmem = pl.BlockSpec(memory_space=pltpu.VMEM)
    (ug, ud), (cg, cd) = UNITS, WIDTHS
    dma = pltpu.SemaphoreType.DMA
    scratch = [
        pltpu.VMEM((STEPS, 2, ROWS, D), BF16),
        pltpu.VMEM((D, 2 * FF), BF16),
        pltpu.VMEM((FF, D), BF16),
        pltpu.VMEM((1, D), F32),
        pltpu.VMEM((D, 2 * FF), F32),
        pltpu.VMEM((8 * FF, CH), F32),
        pltpu.VMEM((ROWS, D), BF16),
        pltpu.VMEM((ROWS, 2 * FF), F32),
        pltpu.VMEM((ROWS, FF), F32),
        pltpu.VMEM((ROWS, 2 * FF), BF16),
        pltpu.VMEM((ROWS, FF), BF16),
        pltpu.VMEM((STEPS, HALF, D), BF16),
        pltpu.VMEM((2, HALF, D), BF16),
        pltpu.VMEM((STEPS, HALF, D), BF16),
        pltpu.VMEM((2, PIECE, D), BF16),
        pltpu.VMEM((2, PIECE, D), BF16),
        pltpu.VMEM((4, PIECE, D), BF16),
        pltpu.VMEM((4, PIECE, D), BF16),
        pltpu.VMEM((D, cg), BF16),
        pltpu.VMEM((8 * FF, cd), BF16),
        pltpu.VMEM((2, 2, 2 * ug, cg), BF16),
        pltpu.VMEM((2, 2, 2 * ud, cd), BF16),
        pltpu.VMEM((2, 2, 4 * ug, cg), BF16),
        pltpu.VMEM((2, 2, 4 * ud, cd), BF16),
        pltpu.VMEM((2 * 4 * ug, cg), BF16),
        pltpu.VMEM((2 * 4 * ud, cd), BF16),
        pltpu.VMEM((2, 2, ug // 2, cg), BF16),
        pltpu.VMEM((2, 2, ud // 2, cd), BF16),
        pltpu.VMEM((2, 2, ug, cg), BF16),
        pltpu.VMEM((2, 2, ud, cd), BF16),
        pltpu.VMEM((2, ug, cg), BF16),
        pltpu.VMEM((2, ud, cd), BF16),
        pltpu.VMEM((2, 8, D), F32),
        pltpu.VMEM((4, 8, D), F32),
        pltpu.VMEM((4, 8, D), F32),
        pltpu.VMEM((4, 8, D), F32),
        dma((8,)),
        dma((20,)),
        dma((STEPS, 3)),
        dma((2,)),
        dma((STEPS,)),
        dma((14,)),
        dma((3, 4)),
        dma((4, 21)),
        dma((4, 20)),
        dma((10,)),
        dma((10,)),
    ]
    return pl.pallas_call(
        kernel,
        name="fused",
        out_shape=(
            jax.ShapeDtypeStruct((ROWS, D), BF16),
            jax.ShapeDtypeStruct((8, D), F32),
            jax.ShapeDtypeStruct((D, 2 * FF), BF16),
            jax.ShapeDtypeStruct((8 * FF, CH), BF16),
        ),
        in_specs=[any_space] * 6,
        out_specs=(vmem, vmem, any_space, any_space),
        scratch_shapes=scratch,
        compiler_params=pltpu.CompilerParams(
            collective_id=0, has_side_effects=True, vmem_limit_bytes=66_000_000
        ),
    )(tokens_in, norm_gain.reshape(1, D), gate_weight, up_weight, down_weight, out_grad)


def shards(tokens_in, norm_gain, gate_weight, up_weight, down_weight, out_grad):
    row_count = tokens_in.shape[0]
    total_tokens = row_count * lax.axis_size("rep") * lax.axis_size("fs") * lax.axis_size("tp")
    factor = float(total_tokens) ** (-0.5)
    grad_in, gain8, gu, dn = fused(tokens_in, norm_gain, gate_weight, up_weight, down_weight, out_grad)
    grad_gain = jnp.sum(gain8, axis=0)
    grad_gate = gu[:, :FF].astype(F32) * factor
    grad_up = gu[:, FF:].astype(F32) * factor
    grad_down = jnp.swapaxes(dn.reshape(8, FF, CH), 0, 1).reshape(FF, D).astype(F32) * (0.5 * factor)
    return (grad_in, grad_gain, grad_gate, grad_up, grad_down)


def solution(mesh):
    in_specs = (
        P(("rep", "fs", "tp"), None),
        P(),
        P(None, ("fs", "tp")),
        P(None, ("fs", "tp")),
        P(("fs", "tp"), None),
        P(("rep", "fs", "tp"), None),
    )
    out_specs = (
        P(("rep", "fs", "tp"), None),
        P(),
        P(None, ("fs", "tp")),
        P(None, ("fs", "tp")),
        P(("fs", "tp"), None),
    )
    return jax.shard_map(shards, mesh=mesh, in_specs=in_specs, out_specs=out_specs, check_vma=False)
```

```python
import jax
import jax.numpy as jnp
from jax import lax
from jax.experimental import pallas as pl
from jax.experimental.pallas import tpu as pltpu
from jax.sharding import PartitionSpec as P

norm_eps = 1e-06
MESH = pl.DeviceIdType.MESH
scope = jax.named_scope
F32 = jnp.float32
BF16 = jnp.bfloat16

D = 2048
FF = 384
ROWS = 256
PIECE = 64
HALF = 128
STEPS = 8
CH = 256
WIDE = 512
UNITS = (64, 64, 96)
WIDTHS = (FF, FF, CH)


def over(n, step, body):
    def go(i, carry):
        body(pl.multiple_of(i * step, step))
        return carry

    lax.fori_loop(0, n // step, go, 0)


def dot(a, b, ca, cb):
    return lax.dot_general(a, b, (((ca,), (cb,)), ((), ())), preferred_element_type=F32)


def kernel(
    x_in, gain_in, gate_in, up_in, down_in, g_in,
    gin_out, gain_out, ga_out, up_out, dn_out,
    xg, wgu, wdn, wgu_t, gain, acc_gu, acc_dn, pre, gh, dgu, hid,
    kept, away, from_sib, far_l, far_r, near_l, near_r,
    wg, wd, s1g, s1d, t1g, t1d, vg, vd, s2g, s2d, t2g, t2d,
    g_acc, g_tp, g_y, g_rep,
    ld_sem, ag_send, ag_recv, ag7_send, ag7_recv, sib_send, sib_recv, rs_send, rs_recv,
    ar_send, ar_recv, gn_send, gn_recv,
):
    rep, fs, tp = lax.axis_index("rep"), lax.axis_index("fs"), lax.axis_index("tp")
    z, x = rep // 4, rep % 4

    def y_at(k):
        return {"rep": rep, "fs": (fs + k) % 4, "tp": tp}

    def x_at(k):
        return {"rep": z * 4 + (x + k) % 4, "fs": fs, "tp": tp}

    def z_at(k):
        return {"rep": ((z + k) % 4) * 4 + x, "fs": fs, "tp": tp}

    sib = {"rep": rep, "fs": fs, "tp": 1 - tp}

    def remote(src, dst, send, recv, to):
        return pltpu.make_async_remote_copy(
            src_ref=src, dst_ref=dst, send_sem=send, recv_sem=recv, device_id=to, device_id_type=MESH
        )

    loads = []
    for s in range(2):
        loads.append(pltpu.make_async_copy(x_in.at[pl.ds(s * HALF, HALF)], away.at[s], ld_sem.at[2 * s]))
        loads.append(pltpu.make_async_copy(g_in.at[pl.ds(s * HALF, HALF)], xg.at[s, 1, pl.ds(0, HALF)], ld_sem.at[2 * s + 1]))
    loads.append(pltpu.make_async_copy(gate_in, wgu.at[:, pl.ds(0, FF)], ld_sem.at[4]))
    loads.append(pltpu.make_async_copy(up_in, wgu.at[:, pl.ds(FF, FF)], ld_sem.at[5]))
    loads.append(pltpu.make_async_copy(down_in, wdn, ld_sem.at[6]))
    loads.append(pltpu.make_async_copy(gain_in, gain, ld_sem.at[7]))
    for c in loads:
        c.start()

    barrier = pltpu.get_barrier_semaphore()
    plane = [
        {"rep": ((z + k // 4) % 4) * 4 + (x + k % 4) % 4, "fs": fs, "tp": tp} for k in range(1, 16)
    ]
    partners = [sib] + [y_at(k) for k in (1, 3, 2)] + plane
    for p in partners:
        pl.semaphore_signal(barrier, inc=1, device_id=p, device_id_type=MESH)

    def to_sib(s):
        return remote(
            xg.at[s, :, pl.ds(0, HALF)], xg.at[s, :, pl.ds(HALF, HALF)], ag_send.at[s], ag_recv.at[s, 2], sib
        )

    def own_piece(p, j):
        src = xg.at[p // 2, :, pl.ds((p % 2) * PIECE, PIECE)]
        dst = xg.at[2 + p, :, pl.ds(j * PIECE, PIECE)]
        return remote(src, dst, ag_send.at[8 + 2 * p + j], ag_recv.at[2 + p, j], y_at(1 if j == 0 else 3))

    def onward(s, j):
        return remote(
            xg.at[s, :, pl.ds(j * PIECE, PIECE)],
            xg.at[s + 4 - 2 * j, :, pl.ds(j * PIECE, PIECE)],
            ag_send.at[14 + s],
            ag_recv.at[s + 4 - 2 * j, j],
            y_at(1 if j == 0 else 3),
        )

    def last_onward(j, q):
        rows = pl.ds(j * PIECE + q * 32, 32)
        return remote(
            xg.at[3 + 2 * j, :, rows], xg.at[7, :, rows], ag7_send.at[0, j, q], ag7_recv.at[0, j, q], y_at(1 if j == 0 else 3)
        )

    def last_to_sib(j, q):
        near, far = pl.ds(j * PIECE + q * 32, 32), pl.ds(HALF + j * PIECE + q * 32, 32)
        return remote(xg.at[7, :, near], xg.at[7, :, far], ag7_send.at[1, j, q], ag7_recv.at[1, j, q], sib)

    parts = [(j, q) for q in range(2) for j in range(2)]

    def arrival(s, j):
        ref = xg.at[s, :, pl.ds(j * PIECE, PIECE)]
        return remote(ref, ref, ag_send.at[0], ag_recv.at[s, j], sib)

    def norm(p):
        def rows16(i, carry):
            rows = pl.ds(pl.multiple_of((p % 2) * PIECE + i * 16, 16), 16)
            floats = away[p // 2, rows, :].astype(F32)
            inverse = lax.rsqrt(jnp.mean(floats * floats, axis=-1, keepdims=True) + norm_eps)
            xg[p // 2, 0, rows, :] = (floats * inverse * gain[...]).astype(BF16)
            return carry

        lax.fori_loop(0, PIECE // 16, rows16, 0, unroll=2)

    def leave(p):
        own_piece(p, 0).start()
        own_piece(p, 1).start()

    with scope("first"):
        loads[7].wait()
        loads[0].wait()
        norm(0)
        loads[1].wait()
    with scope("barrier"):
        pl.semaphore_wait(barrier, len(partners))
    leave(0)
    norm(1)
    loads[2].wait()
    norm(2)
    to_sib(0).start()
    leave(1)
    norm(3)
    loads[3].wait()
    leave(2)
    for c in loads[4:7]:
        c.wait()
    to_sib(1).start()
    leave(3)

    def turn(c):
        cols = pl.ds(c, CH)
        wgu_t[:, cols] = wgu[cols, :].T

    with scope("turn"):
        over(D, CH, turn)

    def zero(r):
        acc_gu[pl.ds(r, 64), :] = jnp.zeros((64, 2 * FF), F32)
        acc_dn[pl.ds(pl.multiple_of(r // 64 * 96, 96), 96), :] = jnp.zeros((96, CH), F32)

    with scope('zero'):
        over(D, 64, zero)

    def sib_sum(s):
        return remote(away.at[s % 2], from_sib.at[s], sib_send.at[s % 2], sib_recv.at[s], sib)

    def chip_sum(s):
        sib_sum(s).wait_recv()

        def add(r):
            rows = pl.ds(r, 32)
            kept[s, rows, :] = (kept[s, rows, :].astype(F32) + from_sib[s, rows, :].astype(F32)).astype(BF16)

        over(HALF, 32, add)

    def early_right(q):
        return remote(kept.at[q, pl.ds(PIECE, PIECE)], near_l.at[q - 2], rs_send.at[q], rs_recv.at[0, q - 2], y_at(1))

    def early_left(q):
        return remote(kept.at[q, pl.ds(0, PIECE)], near_r.at[q - 2], rs_send.at[q], rs_recv.at[1, q - 2], y_at(3))

    def far_left(q):
        return remote(kept.at[q, pl.ds(0, PIECE)], far_r.at[q - 6], rs_send.at[q], rs_recv.at[2, q - 6], y_at(3))

    def far_right(q):
        return remote(kept.at[q, pl.ds(PIECE, PIECE)], far_l.at[q - 6], rs_send.at[q + 2], rs_recv.at[2, q - 4], y_at(1))

    def late_left(q):
        return remote(kept.at[q, pl.ds(0, PIECE)], near_r.at[q - 2], rs_send.at[q + 8], rs_recv.at[1, q - 2], y_at(3))

    def late_right(q):
        return remote(kept.at[q, pl.ds(PIECE, PIECE)], near_l.at[q - 2], rs_send.at[q + 8], rs_recv.at[0, q - 2], y_at(1))

    packed = [(*(ref.at[k] for ref in (wg, s1g, t1g, vg, s2g, t2g)), out) for k, out in enumerate((ga_out, up_out))]
    packed.append((wd, s1d, t1d, vd, s2d, t2d, dn_out))
    halves = ((x, z, x_at, z_at), (z, x, z_at, x_at))
    streams = [(h, k) for k in range(3) for h in range(2)]

    class Ring:
        def __init__(self, h, k, src, base, size, mid, end, index, at, sem):
            self.src, self.size, self.mid, self.end = src, size, mid, end
            half = size // 2
            self.half = half
            f = h * 3 + k

            def rows(chunk, part):
                start = base + ((index + chunk) % 4) * size + part * half
                return pl.ds(pl.multiple_of(start, 16), half)

            self.rows = rows

            def copy(i, chunk, part, dst, to):
                return remote(src.at[rows(chunk, part)], dst, ar_send.at[f, sem + i], ar_recv.at[f, sem + i], at(to))

            self.first = [
                copy(0, 2, 0, mid.at[h, 1], 3),
                copy(1, 2, 1, mid.at[h, 0], 1),
                copy(2, 3, 1, end.at[h, 1, pl.ds(half, half)], 3),
                copy(3, 1, 0, end.at[h, 0, pl.ds(0, half)], 1),
            ]
            self.second = [
                copy(4, 3, 0, end.at[h, 1, pl.ds(0, half)], 3),
                copy(5, 1, 1, end.at[h, 0, pl.ds(half, half)], 1),
            ]
            self.h = h

        def issue(self):
            for c in self.first:
                c.start()

        def relay(self):
            h = self.h
            for i, (chunk, part, side) in enumerate(((3, 0, 1), (1, 1, 0))):
                self.first[i].wait_recv()
                rows = self.rows(chunk, part)
                self.src[rows, :] = (self.src[rows, :].astype(F32) + self.mid[h, side].astype(F32)).astype(BF16)
                self.second[i].start()

        def finish(self, store):
            h = self.h
            for c in self.first[2:] + self.second:
                c.wait_recv()
            for part in range(2):
                local = pl.ds(part * self.half, self.half)
                total = self.src[self.rows(0, part), :].astype(F32)
                total = total + self.end[h, 0, local, :].astype(F32) + self.end[h, 1, local, :].astype(F32)
                store(part, total.astype(BF16))

        def drain(self):
            for c in self.first + self.second:
                c.wait_send()

    rings1, rings2 = {}, {}
    for h, k in streams:
        w, s1, t1, v, s2, t2, out = packed[k]
        i1, i2, at1, at2 = halves[h]
        unit = UNITS[k]
        rings1[h, k] = Ring(h, k, w, h * 16 * unit, 4 * unit, s1, t1, i1, at1, 0)
        rings2[h, k] = Ring(h, k, v, h * 4 * unit, unit, s2, t2, i2, at2, 6)

    def step(s, carry):
        with scope("w_sib"):

            @pl.when(s < STEPS - 1)
            def _():
                to_sib(s).wait_recv()

            @pl.when(s == STEPS - 1)
            def _():
                for j, q in parts:
                    last_to_sib(j, q).wait_recv()

        with scope("pre"):
            pre[...] = dot(xg[s, 0], wgu[...], 1, 0)
        with scope("gh"):
            gh[...] = dot(xg[s, 1], wdn[...], 1, 1)

        def gates(r):
            rows = pl.ds(r, 32)
            gate_pre, up_pre = pre[rows, :FF], pre[rows, FF:]
            grad_hidden = 0.5 * gh[rows, :]
            sigma = jax.nn.sigmoid(gate_pre)
            active = gate_pre * sigma
            hid[rows, :] = (active * up_pre).astype(BF16)
            dgu[rows, :FF] = (grad_hidden * up_pre * sigma * (1.0 + gate_pre * (1.0 - sigma))).astype(BF16)
            dgu[rows, FF:] = (grad_hidden * active).astype(BF16)

        with scope("gates"):
            over(ROWS, 32, gates)

        def part_gu(c):
            cols = pl.ds(c, WIDE)
            return cols, acc_gu[cols, :] + dot(xg[s, 0, :, cols], dgu[...], 0, 0)

        def part_dn(c, store):
            value = dot(hid[...], xg[s, 1, :, pl.ds(c, WIDE)], 0, 0)
            for i in range(WIDE // CH):
                rows = pl.ds(pl.multiple_of((c // CH + i) * FF, FF), FF)
                store(rows, acc_dn[rows, :] + value[:, i * CH : (i + 1) * CH])

        @pl.when(s < STEPS - 1)
        def _():
            def keep_dn(rows, value):
                acc_dn[rows, :] = value

            def weights(c):
                cols, value = part_gu(c)
                acc_gu[cols, :] = value
                part_dn(c, keep_dn)

            with scope("weights"):
                over(D, WIDE, weights)

        @pl.when(s == STEPS - 1)
        def _():
            def last_gu(c):
                cols, value = part_gu(c)
                wg[0, cols, :] = value[:, :FF].astype(BF16)
                wg[1, cols, :] = value[:, FF:].astype(BF16)

            def last_dn(rows, value):
                wd[rows, :] = value.astype(BF16)

            for h in range(2):
                with scope("last_gu"):
                    over(D // 2, WIDE, lambda c: last_gu(c + h * (D // 2)))
                rings1[h, 0].issue()
            with scope("last_dn"):
                over(D, WIDE, lambda c: part_dn(c, last_dn))
            for h in range(2):
                with scope("relay10"):
                    rings1[h, 0].relay()
                rings1[h, 1].issue()

        @pl.when((s >= 1) & (s < STEPS - 2))
        def _():
            with scope("w_nbr"):
                arrival(s + 1, 0).wait_recv()
                arrival(s + 1, 1).wait_recv()
            to_sib(s + 1).start()

        @pl.when(s == STEPS - 2)
        def _():
            with scope("w_nbr"):
                for j, q in parts:
                    last_onward(j, q).wait_recv()
                    last_to_sib(j, q).start()

        @pl.when(s == 1)
        def _():
            onward(s + 1, 0).start()

        @pl.when(s == 3)
        def _():
            onward(s + 1, 1).start()

        @pl.when(s == 2)
        def _():
            for q in range(2):
                last_onward(0, q).start()

        @pl.when(s == 4)
        def _():
            for q in range(2):
                last_onward(1, q).start()

        @pl.when(s >= 2)
        def _():
            sib_sum(s).wait_send()

        def terms(c):
            cols = pl.ds(c, WIDE)
            term = dot(dgu[...], wgu_t[:, cols], 1, 0).astype(BF16)
            kept[s, :, cols] = term[:HALF]
            away[s % 2, :, cols] = term[HALF:]

        with scope("terms"):
            over(D, WIDE, terms)

        @pl.when(s >= 1)
        def _():
            with scope("chipsum"):
                chip_sum(s - 1)

        sib_sum(s).start()

        @pl.when((s == 3) | (s == 4))
        def _():
            early_right(s - 1).start()

        @pl.when((s == 5) | (s == 6))
        def _():
            early_left(s - 1).start()

        return carry

    lax.fori_loop(0, STEPS, step, 0)

    def add_far(q, lo, far, wait):
        wait.wait_recv()

        def add(r):
            rows = pl.ds(lo + r, 32)
            kept[q, rows, :] = (kept[q, rows, :].astype(F32) + far[pl.ds(r, 32), :].astype(F32)).astype(BF16)

        over(PIECE, 32, add)

    def store_v(h, k):
        v, unit = packed[k][3], UNITS[k]

        def store(part, value):
            v[pl.ds(h * 4 * unit + part * 2 * unit, 2 * unit), :] = value

        return store

    class Back:
        def __init__(self, h, k):
            i1, i2, at1, at2 = halves[h]
            out, f, unit = packed[k][6], h * 3 + k, UNITS[k]
            half = unit // 2

            def spot(ra, rb, part=None):
                a, b = (i1 + ra) % 4, (i2 + rb) % 4
                rows = half if part is not None else unit
                if k < 2:
                    start = ((h * 4 + a) * 4 + b) * unit + (part or 0) * half
                    return pl.ds(pl.multiple_of(start, 16), rows), slice(None)
                start = b * unit + (part or 0) * half
                return pl.ds(pl.multiple_of(start, 16), rows), pl.ds(pl.multiple_of((h * 4 + a) * CH, CH), CH)

            def copy(i, to, *where):
                view = out.at[spot(*where)]
                return remote(view, view, ar_send.at[f, 12 + i], ar_recv.at[f, 12 + i], to)

            self.out, self.spot = out, spot
            self.own2 = [copy(0, at2(1), 0, 0), copy(1, at2(3), 0, 0)]
            self.near2 = [copy(0, at2(1), 0, 3), copy(1, at2(3), 0, 1)]
            self.on2 = [copy(2, at2(1), 0, 3, 0), copy(3, at2(3), 0, 1, 1)]
            self.far2 = [copy(2, at2(1), 0, 2, 0), copy(3, at2(3), 0, 2, 1)]
            self.out1 = [[copy(4 + 2 * r, at1(1), 0, r), copy(5 + 2 * r, at1(3), 0, r)] for r in range(4)]
            self.left1 = [copy(4 + 2 * r, at1(1), 3, r) for r in range(4)]
            self.right1 = [copy(5 + 2 * r, at1(3), 1, r) for r in range(4)]
            self.on1 = {
                0: copy(12, at1(1), 3, 0),
                3: copy(13, at1(1), 3, 3),
                1: copy(14, at1(3), 1, 1),
                2: copy(15, at1(3), 1, 2),
            }
            self.far1 = [copy(i, at1(1), 2, r) for i, r in ((12, 0), (13, 3), (14, 1), (15, 2))]

        def store(self, part, value):
            self.out[self.spot(0, 0, part)] = value

        def send(self, r):
            for c in self.out1[r]:
                c.start()

        def begin(self):
            for c in self.own2:
                c.start()
            self.send(0)

        def middle(self):
            for near, on, r in zip(self.near2, self.on2, (3, 1)):
                near.wait_recv()
                on.start()
                self.send(r)

        def last(self):
            for c in self.far2:
                c.wait_recv()
            self.send(2)

        def pass_on(self, *which):
            for r in which:
                (self.left1 if r in (0, 3) else self.right1)[r].wait_recv()
                self.on1[r].start()

        def finish(self):
            for c in (self.left1[1], self.left1[2], self.right1[0], self.right1[3], *self.far1):
                c.wait_recv()

        def drain(self):
            for c in self.own2 + self.on2 + sum(self.out1, []) + list(self.on1.values()):
                c.wait_send()

    back = {(h, k): Back(h, k) for h, k in streams}

    def own_rows(i, carry):
        r = pl.multiple_of(i * 16, 16)
        s, p = i // 8, i // 4
        half, piece = pl.ds(pl.multiple_of((i % 8) * 16, 16), 16), pl.ds(pl.multiple_of((i % 4) * 16, 16), 16)
        grad = kept[s, half, :].astype(F32) + near_l[p, piece, :].astype(F32) + near_r[p, piece, :].astype(F32)
        floats = away[s, half, :].astype(F32)
        inverse = lax.rsqrt(jnp.mean(floats * floats, axis=-1, keepdims=True) + norm_eps)
        unit_rows = floats * inverse
        gained = grad * unit_rows
        g_acc[...] += gained[:8] + gained[8:]
        scaled = grad * gain[...]
        mean = jnp.mean(scaled * unit_rows, axis=-1, keepdims=True)
        result = xg[s, 1, half, :].astype(F32) + inverse * scaled - unit_rows * inverse * mean
        gin_out[pl.ds(r, 16), :] = result.astype(BF16)
        return carry


    gains = []

    def spread(buffer, index, targets, first):
        copies = [
            remote(buffer.at[index], buffer.at[index], gn_send.at[first + i], gn_recv.at[first + i], to)
            for i, to in enumerate(targets)
        ]
        gains.extend(copies)
        for c in copies:
            c.start()
        return copies

    def both(k, act):
        for h in range(2):
            act(h, k)

    def relay1(h, k):
        rings1[h, k].relay()

    def finish1(h, k):
        rings1[h, k].finish(store_v(h, k))
        rings2[h, k].issue()

    def relay2(h, k):
        rings2[h, k].relay()

    def finish2(h, k):
        rings2[h, k].finish(back[h, k].store)
        back[h, k].begin()

    def near2(h, k):
        back[h, k].middle()

    def far2(h, k):
        back[h, k].last()

    def pass0(h, k):
        back[h, k].pass_on(0)

    def pass1(h, k):
        back[h, k].pass_on(3, 1)

    def pass2(h, k):
        back[h, k].pass_on(2)

    def far1(h, k):
        back[h, k].finish()

    def run(name, k, act):
        with scope(f"{name}{k}"):
            both(k, act)

    far_left(6).start()
    far_right(6).start()
    with scope("chip7"):
        chip_sum(7)
    far_left(7).start()
    far_right(7).start()
    sib_sum(6).wait_send()
    sib_sum(7).wait_send()
    again = [pltpu.make_async_copy(x_in.at[pl.ds(s * HALF, HALF)], away.at[s], ld_sem.at[s]) for s in range(2)]
    for c in again:
        c.start()

    def far(i):
        with scope("far"):
            add_far(2 + i, 0, far_r.at[i], far_left(6 + i))
            late_left(2 + i).start()
            add_far(4 + i, PIECE, far_l.at[i], far_right(6 + i))
            late_right(4 + i).start()

    run("finish1", 0, finish1)
    for h in range(2):
        with scope("relay11"):
            rings1[h, 1].relay()
    run("relay2", 0, relay2)
    both(2, lambda h, k: rings1[h, k].issue())
    run("finish1", 1, finish1)
    far(0)
    run("finish2", 0, finish2)
    run("relay2", 1, relay2)
    run("near2", 0, near2)
    run("relay1", 2, relay1)
    run("pass0", 0, pass0)
    run("finish2", 1, finish2)
    run("far2", 0, far2)
    far(1)
    run("finish1", 2, finish1)
    run("near2", 1, near2)
    run("pass1", 0, pass1)
    run("pass0", 1, pass0)
    run("relay2", 2, relay2)
    run("far2", 1, far2)
    run("pass2", 0, pass2)
    run("finish2", 2, finish2)
    run("pass1", 1, pass1)
    with scope("w_rs"):
        for c in again:
            c.wait()
        for q in (2, 3):
            early_right(q).wait_recv()
            late_left(q).wait_recv()
        for q in (4, 5):
            early_left(q).wait_recv()
            late_right(q).wait_recv()
    with scope("own"):
        g_acc[...] = jnp.zeros((8, D), F32)
        lax.fori_loop(0, ROWS // 16, own_rows, 0, unroll=2)
        g_tp[tp] = jnp.sum(g_acc[...], axis=0, keepdims=True)
    g1 = spread(g_tp, tp, [sib], 0)
    run("near2", 2, near2)
    run("pass2", 1, pass2)
    with scope("g1"):
        g1[0].wait_recv()
        g_y[fs] = g_tp[0] + g_tp[1]
        g2 = spread(g_y, fs, [y_at(1), y_at(2), y_at(3)], 1)
    run("far2", 2, far2)
    run("pass0", 2, pass0)
    with scope("g2"):
        for c in g2:
            c.wait_recv()
        g_rep[rep] = (g_y[0] + g_y[1]) + (g_y[2] + g_y[3])
        g3 = spread(g_rep, rep, plane, 4)
    run("pass1", 2, pass1)
    run("pass2", 2, pass2)
    with scope("g3"):
        for c in g3:
            c.wait_recv()
        total = g_rep[0]
        for i in range(1, 16):
            total = total + g_rep[i]
        gain_out[...] = total
    run("far1", 0, far1)
    run("far1", 1, far1)
    run("far1", 2, far1)

    for s in range(STEPS - 1):
        to_sib(s).wait_send()
    for p in range(4):
        own_piece(p, 0).wait_send()
        own_piece(p, 1).wait_send()
    for s in (2, 4):
        onward(s, 0 if s < 4 else 1).wait_send()
    for j, q in parts:
        last_onward(j, q).wait_send()
        last_to_sib(j, q).wait_send()
    for q in (2, 3):
        early_right(q).wait_send()
        late_left(q).wait_send()
    for q in (4, 5):
        early_left(q).wait_send()
        late_right(q).wait_send()
    for q in (6, 7):
        far_left(q).wait_send()
        far_right(q).wait_send()
    for h, k in streams:
        rings1[h, k].drain()
        rings2[h, k].drain()
        back[h, k].drain()
    for c in gains:
        c.wait_send()


def fused(tokens_in, norm_gain, gate_weight, up_weight, down_weight, out_grad):
    any_space = pl.BlockSpec(memory_space=pl.ANY)
    vmem = pl.BlockSpec(memory_space=pltpu.VMEM)
    (ug, _, ud), (cg, _, cd) = UNITS, WIDTHS
    dma = pltpu.SemaphoreType.DMA
    scratch = [
        pltpu.VMEM((STEPS, 2, ROWS, D), BF16),
        pltpu.VMEM((D, 2 * FF), BF16),
        pltpu.VMEM((FF, D), BF16),
        pltpu.VMEM((2 * FF, D), BF16),
        pltpu.VMEM((1, D), F32),
        pltpu.VMEM((D, 2 * FF), F32),
        pltpu.VMEM((8 * FF, CH), F32),
        pltpu.VMEM((ROWS, 2 * FF), F32),
        pltpu.VMEM((ROWS, FF), F32),
        pltpu.VMEM((ROWS, 2 * FF), BF16),
        pltpu.VMEM((ROWS, FF), BF16),
        pltpu.VMEM((STEPS, HALF, D), BF16),
        pltpu.VMEM((2, HALF, D), BF16),
        pltpu.VMEM((STEPS, HALF, D), BF16),
        pltpu.VMEM((2, PIECE, D), BF16),
        pltpu.VMEM((2, PIECE, D), BF16),
        pltpu.VMEM((4, PIECE, D), BF16),
        pltpu.VMEM((4, PIECE, D), BF16),
        pltpu.VMEM((2, D, cg), BF16),
        pltpu.VMEM((8 * FF, cd), BF16),
        pltpu.VMEM((2, 2, 2, 2 * ug, cg), BF16),
        pltpu.VMEM((2, 2, 2 * ud, cd), BF16),
        pltpu.VMEM((2, 2, 2, 4 * ug, cg), BF16),
        pltpu.VMEM((2, 2, 4 * ud, cd), BF16),
        pltpu.VMEM((2, 2 * 4 * ug, cg), BF16),
        pltpu.VMEM((2 * 4 * ud, cd), BF16),
        pltpu.VMEM((2, 2, 2, ug // 2, cg), BF16),
        pltpu.VMEM((2, 2, ud // 2, cd), BF16),
        pltpu.VMEM((2, 2, 2, ug, cg), BF16),
        pltpu.VMEM((2, 2, ud, cd), BF16),
        pltpu.VMEM((8, D), F32),
        pltpu.VMEM((2, 1, D), F32),
        pltpu.VMEM((4, 1, D), F32),
        pltpu.VMEM((16, 1, D), F32),
        dma((8,)),
        dma((20,)),
        dma((STEPS, 3)),
        dma((2, 2, 2)),
        dma((2, 2, 2)),
        dma((2,)),
        dma((STEPS,)),
        dma((14,)),
        dma((3, 4)),
        dma((6, 28)),
        dma((6, 28)),
        dma((19,)),
        dma((19,)),
    ]
    return pl.pallas_call(
        kernel,
        name="fused",
        out_shape=(
            pltpu.VMEM((ROWS, D), BF16),
            pltpu.VMEM((1, D), F32),
            pltpu.VMEM((D, FF), BF16),
            pltpu.VMEM((D, FF), BF16),
            pltpu.VMEM((FF, D), BF16),
        ),
        in_specs=[any_space] * 6,
        out_specs=(vmem,) * 5,
        scratch_shapes=scratch,
        compiler_params=pltpu.CompilerParams(
            collective_id=0, has_side_effects=True, vmem_limit_bytes=60_800_000
        ),
    )(tokens_in, norm_gain.reshape(1, D), gate_weight, up_weight, down_weight, out_grad)


def shards(tokens_in, norm_gain, gate_weight, up_weight, down_weight, out_grad):
    row_count = tokens_in.shape[0]
    total_tokens = row_count * lax.axis_size("rep") * lax.axis_size("fs") * lax.axis_size("tp")
    factor = float(total_tokens) ** (-0.5)
    grad_in, gain_row, ga, up, dn = fused(tokens_in, norm_gain, gate_weight, up_weight, down_weight, out_grad)
    grad_gain = gain_row.reshape(D)
    grad_gate = ga.astype(F32) * factor
    grad_up = up.astype(F32) * factor
    grad_down = dn.astype(F32) * (0.5 * factor)
    return (grad_in, grad_gain, grad_gate, grad_up, grad_down)


def solution(mesh):
    in_specs = (
        P(("rep", "fs", "tp"), None),
        P(),
        P(None, ("fs", "tp")),
        P(None, ("fs", "tp")),
        P(("fs", "tp"), None),
        P(("rep", "fs", "tp"), None),
    )
    out_specs = (
        P(("rep", "fs", "tp"), None),
        P(),
        P(None, ("fs", "tp")),
        P(None, ("fs", "tp")),
        P(("fs", "tp"), None),
    )
    return jax.shard_map(shards, mesh=mesh, in_specs=in_specs, out_specs=out_specs, check_vma=False)
```

```python
import functools

import jax
import jax.numpy as jnp
from jax import lax
from jax.experimental import pallas as pl
from jax.experimental.pallas import tpu as pltpu
from jax.sharding import PartitionSpec as P

norm_eps = 1e-06
MESH = pl.DeviceIdType.MESH
scope = jax.named_scope
F32 = jnp.float32
BF16 = jnp.bfloat16

D = 2048
FF = 384
ROWS = 256
PIECE = 64
HALF = 128
STEPS = 8
CH = 256
WIDE = 512
UNITS = (64, 64, 96)
WIDTHS = (FF, FF, CH)


def over(n, step, body):
    def go(i, carry):
        body(pl.multiple_of(i * step, step))
        return carry

    lax.fori_loop(0, n // step, go, 0)


def dot(a, b, ca, cb):
    return lax.dot_general(a, b, (((ca,), (cb,)), ((), ())), preferred_element_type=F32)


def kernel(
    x_in, gain_in, gate_in, up_in, down_in, g_in,
    gin_out, gain_out, ga_out, up_out, dn_out,
    xg, wgu, wdn, wgu_t, gain, acc_gu, acc_dn, pre, gh, dgu, hid,
    kept, away, from_sib, far_l, far_r, near_l, near_r,
    wg, wd, s1g, s1d, t1g, t1d, vg, vd, s2g, s2d, t2g, t2d,
    g_acc, g_tp, g_y, g_rep,
    ld_sem, ag_send, ag_recv, ag7_send, ag7_recv, sib_send, sib_recv, rs_send, rs_recv,
    ar_send, ar_recv, gn_send, gn_recv,
):
    rep, fs, tp = lax.axis_index("rep"), lax.axis_index("fs"), lax.axis_index("tp")
    z, x = rep // 4, rep % 4

    def y_at(k):
        return {"rep": rep, "fs": (fs + k) % 4, "tp": tp}

    def x_at(k):
        return {"rep": z * 4 + (x + k) % 4, "fs": fs, "tp": tp}

    def z_at(k):
        return {"rep": ((z + k) % 4) * 4 + x, "fs": fs, "tp": tp}

    sib = {"rep": rep, "fs": fs, "tp": 1 - tp}

    def remote(src, dst, send, recv, to):
        return pltpu.make_async_remote_copy(
            src_ref=src, dst_ref=dst, send_sem=send, recv_sem=recv, device_id=to, device_id_type=MESH
        )

    loads = []
    for s in range(2):
        loads.append(pltpu.make_async_copy(x_in.at[pl.ds(s * HALF, HALF)], away.at[s], ld_sem.at[2 * s]))
        loads.append(pltpu.make_async_copy(g_in.at[pl.ds(s * HALF, HALF)], xg.at[s, 1, pl.ds(0, HALF)], ld_sem.at[2 * s + 1]))
    loads.append(pltpu.make_async_copy(gate_in, wgu.at[:, pl.ds(0, FF)], ld_sem.at[4]))
    loads.append(pltpu.make_async_copy(up_in, wgu.at[:, pl.ds(FF, FF)], ld_sem.at[5]))
    loads.append(pltpu.make_async_copy(down_in, wdn, ld_sem.at[6]))
    loads.append(pltpu.make_async_copy(gain_in, gain, ld_sem.at[7]))
    for i in (7, 0, 1, 2, 3):
        loads[i].start()

    barrier = pltpu.get_barrier_semaphore()
    plane = [
        {"rep": ((z + k // 4) % 4) * 4 + (x + k % 4) % 4, "fs": fs, "tp": tp} for k in range(1, 16)
    ]
    partners = [sib] + [y_at(k) for k in (1, 3, 2)] + plane
    for p in partners:
        pl.semaphore_signal(barrier, inc=1, device_id=p, device_id_type=MESH)

    def to_sib(s):
        return remote(
            xg.at[s, :, pl.ds(0, HALF)], xg.at[s, :, pl.ds(HALF, HALF)], ag_send.at[s], ag_recv.at[s, 2], sib
        )

    def own_piece(p, j):
        src = xg.at[p // 2, :, pl.ds((p % 2) * PIECE, PIECE)]
        dst = xg.at[2 + p, :, pl.ds(j * PIECE, PIECE)]
        return remote(src, dst, ag_send.at[8 + 2 * p + j], ag_recv.at[2 + p, j], y_at(1 if j == 0 else 3))

    def onward(s, j):
        return remote(
            xg.at[s, :, pl.ds(j * PIECE, PIECE)],
            xg.at[s + 4 - 2 * j, :, pl.ds(j * PIECE, PIECE)],
            ag_send.at[14 + s],
            ag_recv.at[s + 4 - 2 * j, j],
            y_at(1 if j == 0 else 3),
        )

    def last_onward(j, q):
        rows = pl.ds(j * PIECE + q * 32, 32)
        return remote(
            xg.at[3 + 2 * j, :, rows], xg.at[7, :, rows], ag7_send.at[0, j, q], ag7_recv.at[0, j, q], y_at(1 if j == 0 else 3)
        )

    def last_to_sib(j, q):
        near, far = pl.ds(j * PIECE + q * 32, 32), pl.ds(HALF + j * PIECE + q * 32, 32)
        return remote(xg.at[7, :, near], xg.at[7, :, far], ag7_send.at[1, j, q], ag7_recv.at[1, j, q], sib)

    parts = [(j, q) for q in range(2) for j in range(2)]

    def arrival(s, j):
        ref = xg.at[s, :, pl.ds(j * PIECE, PIECE)]
        return remote(ref, ref, ag_send.at[0], ag_recv.at[s, j], sib)

    def norm(p):
        def rows16(i, carry):
            rows = pl.ds(pl.multiple_of((p % 2) * PIECE + i * 16, 16), 16)
            floats = away[p // 2, rows, :].astype(F32)
            inverse = lax.rsqrt(jnp.mean(floats * floats, axis=-1, keepdims=True) + norm_eps)
            xg[p // 2, 0, rows, :] = (floats * inverse * gain[...]).astype(BF16)
            return carry

        lax.fori_loop(0, PIECE // 16, rows16, 0, unroll=2)

    def leave(p):
        own_piece(p, 0).start()
        own_piece(p, 1).start()

    with scope("first"):
        loads[7].wait()
        loads[0].wait()
        loads[1].wait()
        for c in loads[4:7]:
            c.start()
        norm(0)
    with scope("barrier"):
        pl.semaphore_wait(barrier, len(partners))
    leave(0)
    norm(1)
    loads[2].wait()
    norm(2)
    to_sib(0).start()
    leave(1)
    norm(3)
    loads[3].wait()
    leave(2)
    for c in loads[4:7]:
        c.wait()
    to_sib(1).start()
    leave(3)

    def turn(c):
        cols = pl.ds(c, CH)
        wgu_t[:, cols] = wgu[cols, :].T

    with scope("turn"):
        over(D, CH, turn)

    def zero(r):
        acc_gu[pl.ds(r, 64), :] = jnp.zeros((64, 2 * FF), F32)
        acc_dn[pl.ds(pl.multiple_of(r // 64 * 96, 96), 96), :] = jnp.zeros((96, CH), F32)

    with scope('zero'):
        over(D, 64, zero)

    def sib_sum(s):
        return remote(away.at[s % 2], from_sib.at[s], sib_send.at[s % 2], sib_recv.at[s], sib)

    def chip_sum(s):
        sib_sum(s).wait_recv()

        def add(r):
            rows = pl.ds(r, 32)
            kept[s, rows, :] = (kept[s, rows, :].astype(F32) + from_sib[s, rows, :].astype(F32)).astype(BF16)

        over(HALF, 32, add)

    def early_right(q):
        return remote(kept.at[q, pl.ds(PIECE, PIECE)], near_l.at[q - 2], rs_send.at[q], rs_recv.at[0, q - 2], y_at(1))

    def early_left(q):
        return remote(kept.at[q, pl.ds(0, PIECE)], near_r.at[q - 2], rs_send.at[q], rs_recv.at[1, q - 2], y_at(3))

    def far_left(q):
        return remote(kept.at[q, pl.ds(0, PIECE)], far_r.at[q - 6], rs_send.at[q], rs_recv.at[2, q - 6], y_at(3))

    def far_right(q):
        return remote(kept.at[q, pl.ds(PIECE, PIECE)], far_l.at[q - 6], rs_send.at[q + 2], rs_recv.at[2, q - 4], y_at(1))

    def late_left(q):
        return remote(kept.at[q, pl.ds(0, PIECE)], near_r.at[q - 2], rs_send.at[q + 8], rs_recv.at[1, q - 2], y_at(3))

    def late_right(q):
        return remote(kept.at[q, pl.ds(PIECE, PIECE)], near_l.at[q - 2], rs_send.at[q + 8], rs_recv.at[0, q - 2], y_at(1))

    packed = [(*(ref.at[k] for ref in (wg, s1g, t1g, vg, s2g, t2g)), out) for k, out in enumerate((ga_out, up_out))]
    packed.append((wd, s1d, t1d, vd, s2d, t2d, dn_out))
    halves = ((x, z, x_at, z_at), (z, x, z_at, x_at))
    streams = [(h, k) for k in range(3) for h in range(2)]

    class Ring:
        def __init__(self, h, k, src, base, size, mid, end, index, at, sem):
            self.src, self.size, self.mid, self.end = src, size, mid, end
            half = size // 2
            self.half = half
            f = h * 3 + k

            def rows(chunk, part):
                start = base + ((index + chunk) % 4) * size + part * half
                return pl.ds(pl.multiple_of(start, 16), half)

            self.rows = rows

            def copy(i, chunk, part, dst, to):
                return remote(src.at[rows(chunk, part)], dst, ar_send.at[f, sem + i], ar_recv.at[f, sem + i], at(to))

            self.first = [
                copy(0, 2, 0, mid.at[h, 1], 3),
                copy(1, 2, 1, mid.at[h, 0], 1),
                copy(2, 3, 1, end.at[h, 1, pl.ds(half, half)], 3),
                copy(3, 1, 0, end.at[h, 0, pl.ds(0, half)], 1),
            ]
            self.second = [
                copy(4, 3, 0, end.at[h, 1, pl.ds(0, half)], 3),
                copy(5, 1, 1, end.at[h, 0, pl.ds(half, half)], 1),
            ]
            self.h = h

        def mid_out(self):
            for c in self.first[:2]:
                c.start()

        def end_out(self):
            for c in self.first[2:]:
                c.start()

        def relay(self):
            h = self.h
            for i, (chunk, part, side) in enumerate(((3, 0, 1), (1, 1, 0))):
                self.first[i].wait_recv()
                rows = self.rows(chunk, part)
                self.src[rows, :] = (self.src[rows, :].astype(F32) + self.mid[h, side].astype(F32)).astype(BF16)
                self.second[i].start()

        def finish(self, store):
            h = self.h
            for c in self.first[2:] + self.second:
                c.wait_recv()
            for part in range(2):
                local = pl.ds(part * self.half, self.half)
                total = self.src[self.rows(0, part), :].astype(F32)
                total = total + self.end[h, 0, local, :].astype(F32) + self.end[h, 1, local, :].astype(F32)
                store(part, total.astype(BF16))

        def drain(self):
            for c in self.first + self.second:
                c.wait_send()

    rings1, rings2 = {}, {}
    for h, k in streams:
        w, s1, t1, v, s2, t2, out = packed[k]
        i1, i2, at1, at2 = halves[h]
        unit = UNITS[k]
        rings1[h, k] = Ring(h, k, w, h * 16 * unit, 4 * unit, s1, t1, i1, at1, 0)
        rings2[h, k] = Ring(h, k, v, h * 4 * unit, unit, s2, t2, i2, at2, 6)

    def step(s, carry):
        with scope("w_sib"):

            @pl.when(s < STEPS - 1)
            def _():
                to_sib(s).wait_recv()

            @pl.when(s == STEPS - 1)
            def _():
                for j, q in parts:
                    last_to_sib(j, q).wait_recv()

        with scope("pre"):
            pre[...] = dot(xg[s, 0], wgu[...], 1, 0)
        with scope("gh"):
            gh[...] = dot(xg[s, 1], wdn[...], 1, 1)

        def gates(r):
            rows = pl.ds(r, 32)
            gate_pre, up_pre = pre[rows, :FF], pre[rows, FF:]
            grad_hidden = 0.5 * gh[rows, :]
            sigma = jax.nn.sigmoid(gate_pre)
            active = gate_pre * sigma
            hid[rows, :] = (active * up_pre).astype(BF16)
            dgu[rows, :FF] = (grad_hidden * up_pre * sigma * (1.0 + gate_pre * (1.0 - sigma))).astype(BF16)
            dgu[rows, FF:] = (grad_hidden * active).astype(BF16)

        with scope("gates"):
            over(ROWS, 32, gates)

        def part_gu(c):
            cols = pl.ds(c, WIDE)
            return cols, acc_gu[cols, :] + dot(xg[s, 0, :, cols], dgu[...], 0, 0)

        def part_dn(c, store):
            value = dot(hid[...], xg[s, 1, :, pl.ds(c, WIDE)], 0, 0)
            for i in range(WIDE // CH):
                rows = pl.ds(pl.multiple_of((c // CH + i) * FF, FF), FF)
                store(rows, acc_dn[rows, :] + value[:, i * CH : (i + 1) * CH])

        @pl.when(s < STEPS - 1)
        def _():
            def keep_dn(rows, value):
                acc_dn[rows, :] = value

            def weights(c):
                cols, value = part_gu(c)
                acc_gu[cols, :] = value
                part_dn(c, keep_dn)

            with scope("weights"):
                over(D, WIDE, weights)

        @pl.when(s == STEPS - 1)
        def _():
            def last_gu(c):
                cols, value = part_gu(c)
                wg[0, cols, :] = value[:, :FF].astype(BF16)
                wg[1, cols, :] = value[:, FF:].astype(BF16)

            def last_dn(rows, value):
                wd[rows, :] = value.astype(BF16)

            for h in range(2):
                with scope("last_gu"):
                    over(D // 2, WIDE, lambda c: last_gu(c + h * (D // 2)))
                rings1[h, 0].mid_out()
                rings1[h, 1].mid_out()
                rings1[h, 0].end_out()
            with scope("last_dn"):
                over(D, WIDE, lambda c: part_dn(c, last_dn))

        @pl.when((s >= 1) & (s < STEPS - 2))
        def _():
            with scope("w_nbr"):
                arrival(s + 1, 0).wait_recv()
                arrival(s + 1, 1).wait_recv()
            to_sib(s + 1).start()

        @pl.when(s == STEPS - 2)
        def _():
            with scope("w_nbr"):
                for j, q in parts:
                    last_onward(j, q).wait_recv()
                    last_to_sib(j, q).start()

        @pl.when(s == 1)
        def _():
            onward(s + 1, 0).start()

        @pl.when(s == 3)
        def _():
            onward(s + 1, 1).start()

        @pl.when(s == 2)
        def _():
            for q in range(2):
                last_onward(0, q).start()

        @pl.when(s == 4)
        def _():
            for q in range(2):
                last_onward(1, q).start()

        @pl.when(s >= 2)
        def _():
            sib_sum(s).wait_send()

        def terms(c):
            cols = pl.ds(c, WIDE)
            term = dot(dgu[...], wgu_t[:, cols], 1, 0).astype(BF16)
            kept[s, :, cols] = term[:HALF]
            away[s % 2, :, cols] = term[HALF:]

        with scope("terms"):
            over(D, WIDE, terms)

        @pl.when(s >= 1)
        def _():
            with scope("chipsum"):
                chip_sum(s - 1)

        sib_sum(s).start()

        @pl.when((s == 3) | (s == 4))
        def _():
            early_right(s - 1).start()

        @pl.when((s == 5) | (s == 6))
        def _():
            early_left(s - 1).start()

        return carry

    lax.fori_loop(0, STEPS, step, 0)

    def add_far(q, lo, far, wait):
        wait.wait_recv()

        def add(r):
            rows = pl.ds(lo + r, 32)
            kept[q, rows, :] = (kept[q, rows, :].astype(F32) + far[pl.ds(r, 32), :].astype(F32)).astype(BF16)

        over(PIECE, 32, add)

    def store_v(h, k):
        v, unit = packed[k][3], UNITS[k]

        def store(part, value):
            v[pl.ds(h * 4 * unit + part * 2 * unit, 2 * unit), :] = value

        return store

    class Back:
        def __init__(self, h, k):
            i1, i2, at1, at2 = halves[h]
            out, f, unit = packed[k][6], h * 3 + k, UNITS[k]
            half = unit // 2

            def spot(ra, rb, part=None):
                a, b = (i1 + ra) % 4, (i2 + rb) % 4
                rows = half if part is not None else unit
                if k < 2:
                    start = ((h * 4 + a) * 4 + b) * unit + (part or 0) * half
                    return pl.ds(pl.multiple_of(start, 16), rows), slice(None)
                start = b * unit + (part or 0) * half
                return pl.ds(pl.multiple_of(start, 16), rows), pl.ds(pl.multiple_of((h * 4 + a) * CH, CH), CH)

            def copy(i, to, *where):
                view = out.at[spot(*where)]
                return remote(view, view, ar_send.at[f, 12 + i], ar_recv.at[f, 12 + i], to)

            self.out, self.spot = out, spot
            self.own2 = [copy(0, at2(1), 0, 0), copy(1, at2(3), 0, 0)]
            self.near2 = [copy(0, at2(1), 0, 3), copy(1, at2(3), 0, 1)]
            self.on2 = [copy(2, at2(1), 0, 3, 0), copy(3, at2(3), 0, 1, 1)]
            self.far2 = [copy(2, at2(1), 0, 2, 0), copy(3, at2(3), 0, 2, 1)]
            self.out1 = [[copy(4 + 2 * r, at1(1), 0, r), copy(5 + 2 * r, at1(3), 0, r)] for r in range(4)]
            self.left1 = [copy(4 + 2 * r, at1(1), 3, r) for r in range(4)]
            self.right1 = [copy(5 + 2 * r, at1(3), 1, r) for r in range(4)]
            self.on1 = {
                0: copy(12, at1(1), 3, 0),
                3: copy(13, at1(1), 3, 3),
                1: copy(14, at1(3), 1, 1),
                2: copy(15, at1(3), 1, 2),
            }
            self.far1 = [copy(i, at1(1), 2, r) for i, r in ((12, 0), (13, 3), (14, 1), (15, 2))]

        def store(self, part, value):
            self.out[self.spot(0, 0, part)] = value

        def send(self, r):
            for c in self.out1[r]:
                c.start()

        def begin(self):
            for c in self.own2:
                c.start()
            self.send(0)

        def middle(self):
            for near, on, r in zip(self.near2, self.on2, (3, 1)):
                near.wait_recv()
                on.start()
                self.send(r)

        def last(self):
            for c in self.far2:
                c.wait_recv()
            self.send(2)

        def pass_on(self, *which):
            for r in which:
                (self.left1 if r in (0, 3) else self.right1)[r].wait_recv()
                self.on1[r].start()

        def finish(self):
            for c in (self.left1[1], self.left1[2], self.right1[0], self.right1[3], *self.far1):
                c.wait_recv()

        def drain(self):
            for c in self.own2 + self.on2 + sum(self.out1, []) + list(self.on1.values()):
                c.wait_send()

    back = {(h, k): Back(h, k) for h, k in streams}

    def own_rows(i, carry):
        r = pl.multiple_of(i * 16, 16)
        s, p = i // 8, i // 4
        half, piece = pl.ds(pl.multiple_of((i % 8) * 16, 16), 16), pl.ds(pl.multiple_of((i % 4) * 16, 16), 16)
        grad = kept[s, half, :].astype(F32) + near_l[p, piece, :].astype(F32) + near_r[p, piece, :].astype(F32)
        floats = away[s, half, :].astype(F32)
        inverse = lax.rsqrt(jnp.mean(floats * floats, axis=-1, keepdims=True) + norm_eps)
        unit_rows = floats * inverse
        gained = grad * unit_rows
        g_acc[...] += gained[:8] + gained[8:]
        scaled = grad * gain[...]
        mean = jnp.mean(scaled * unit_rows, axis=-1, keepdims=True)
        result = xg[s, 1, half, :].astype(F32) + inverse * scaled - unit_rows * inverse * mean
        gin_out[pl.ds(r, 16), :] = result.astype(BF16)
        return carry


    gains = []

    def spread(buffer, index, targets, first):
        copies = [
            remote(buffer.at[index], buffer.at[index], gn_send.at[first + i], gn_recv.at[first + i], to)
            for i, to in enumerate(targets)
        ]
        gains.extend(copies)
        for c in copies:
            c.start()
        return copies

    def both(k, act):
        for h in range(2):
            act(h, k)

    def relay1(h, k):
        rings1[h, k].relay()

    def finish1(h, k):
        rings1[h, k].finish(store_v(h, k))
        rings2[h, k].mid_out()
        rings2[h, k].end_out()

    def relay2(h, k):
        rings2[h, k].relay()

    def finish2(h, k):
        rings2[h, k].finish(back[h, k].store)
        back[h, k].begin()

    def near2(h, k):
        back[h, k].middle()

    def far2(h, k):
        back[h, k].last()

    def pass0(h, k):
        back[h, k].pass_on(0)

    def pass1(h, k):
        back[h, k].pass_on(3, 1)

    def pass2(h, k):
        back[h, k].pass_on(2)

    def far1(h, k):
        back[h, k].finish()

    def run(name, k, act):
        with scope(f"{name}{k}"):
            both(k, act)

    far_left(6).start()
    far_right(6).start()
    with scope("chip7"):
        chip_sum(7)
    far_left(7).start()
    far_right(7).start()
    sib_sum(6).wait_send()
    sib_sum(7).wait_send()
    again = [pltpu.make_async_copy(x_in.at[pl.ds(s * HALF, HALF)], away.at[s], ld_sem.at[s]) for s in range(2)]
    for c in again:
        c.start()

    def far(i):
        with scope("far"):
            add_far(2 + i, 0, far_r.at[i], far_left(6 + i))
            late_left(2 + i).start()
            add_far(4 + i, PIECE, far_l.at[i], far_right(6 + i))
            late_right(4 + i).start()

    run("relay1", 0, relay1)
    run("relay1", 1, relay1)
    both(2, lambda h, k: rings1[h, k].mid_out())
    far(0)
    run("finish1", 0, finish1)
    both(1, lambda h, k: rings1[h, k].end_out())
    both(2, lambda h, k: rings1[h, k].end_out())
    run("relay2", 0, relay2)
    run("relay1", 2, relay1)
    run("finish1", 1, finish1)
    run("finish2", 0, finish2)
    run("finish1", 2, finish1)
    far(1)
    run("relay2", 1, relay2)
    run("near2", 0, near2)
    run("relay2", 2, relay2)
    run("finish2", 1, finish2)
    run("far2", 0, far2)
    run("pass1", 0, pass1)
    run("finish2", 2, finish2)
    run("near2", 1, near2)
    with scope("w_rs"):
        for c in again:
            c.wait()
        for q in (2, 3):
            early_right(q).wait_recv()
            late_left(q).wait_recv()
        for q in (4, 5):
            early_left(q).wait_recv()
            late_right(q).wait_recv()
    with scope("own"):
        g_acc[...] = jnp.zeros((8, D), F32)
        lax.fori_loop(0, ROWS // 16, own_rows, 0, unroll=2)
        g_tp[tp] = jnp.sum(g_acc[...], axis=0, keepdims=True)
    g1 = spread(g_tp, tp, [sib], 0)
    run("near2", 2, near2)
    with scope("g1"):
        g1[0].wait_recv()
        g_y[fs] = g_tp[0] + g_tp[1]
        g2 = spread(g_y, fs, [y_at(1), y_at(2), y_at(3)], 1)
    run("pass2", 0, pass2)
    run("far2", 1, far2)
    with scope("g2"):
        for c in g2:
            c.wait_recv()
        g_rep[rep] = (g_y[0] + g_y[1]) + (g_y[2] + g_y[3])
        g3 = spread(g_rep, rep, plane, 4)
    run("far2", 2, far2)
    run("pass0", 0, pass0)
    run("pass0", 1, pass0)
    run("pass1", 1, pass1)
    run("pass1", 2, pass1)
    run("pass2", 1, pass2)
    run("pass2", 2, pass2)
    run("pass0", 2, pass0)
    with scope("g3"):
        for c in g3:
            c.wait_recv()
        total = g_rep[0]
        for i in range(1, 16):
            total = total + g_rep[i]
        gain_out[...] = total
    run("far1", 0, far1)
    run("far1", 1, far1)
    run("far1", 2, far1)

    for s in range(STEPS - 1):
        to_sib(s).wait_send()
    for p in range(4):
        own_piece(p, 0).wait_send()
        own_piece(p, 1).wait_send()
    for s in (2, 4):
        onward(s, 0 if s < 4 else 1).wait_send()
    for j, q in parts:
        last_onward(j, q).wait_send()
        last_to_sib(j, q).wait_send()
    for q in (2, 3):
        early_right(q).wait_send()
        late_left(q).wait_send()
    for q in (4, 5):
        early_left(q).wait_send()
        late_right(q).wait_send()
    for q in (6, 7):
        far_left(q).wait_send()
        far_right(q).wait_send()
    for h, k in streams:
        rings1[h, k].drain()
        rings2[h, k].drain()
        back[h, k].drain()
    for c in gains:
        c.wait_send()


def fused(tokens_in, norm_gain, gate_weight, up_weight, down_weight, out_grad):
    any_space = pl.BlockSpec(memory_space=pl.ANY)
    vmem = pl.BlockSpec(memory_space=pltpu.VMEM)
    (ug, _, ud), (cg, _, cd) = UNITS, WIDTHS
    dma = pltpu.SemaphoreType.DMA
    scratch = [
        pltpu.VMEM((STEPS, 2, ROWS, D), BF16),
        pltpu.VMEM((D, 2 * FF), BF16),
        pltpu.VMEM((FF, D), BF16),
        pltpu.VMEM((2 * FF, D), BF16),
        pltpu.VMEM((1, D), F32),
        pltpu.VMEM((D, 2 * FF), F32),
        pltpu.VMEM((8 * FF, CH), F32),
        pltpu.VMEM((ROWS, 2 * FF), F32),
        pltpu.VMEM((ROWS, FF), F32),
        pltpu.VMEM((ROWS, 2 * FF), BF16),
        pltpu.VMEM((ROWS, FF), BF16),
        pltpu.VMEM((STEPS, HALF, D), BF16),
        pltpu.VMEM((2, HALF, D), BF16),
        pltpu.VMEM((STEPS, HALF, D), BF16),
        pltpu.VMEM((2, PIECE, D), BF16),
        pltpu.VMEM((2, PIECE, D), BF16),
        pltpu.VMEM((4, PIECE, D), BF16),
        pltpu.VMEM((4, PIECE, D), BF16),
        pltpu.VMEM((2, D, cg), BF16),
        pltpu.VMEM((8 * FF, cd), BF16),
        pltpu.VMEM((2, 2, 2, 2 * ug, cg), BF16),
        pltpu.VMEM((2, 2, 2 * ud, cd), BF16),
        pltpu.VMEM((2, 2, 2, 4 * ug, cg), BF16),
        pltpu.VMEM((2, 2, 4 * ud, cd), BF16),
        pltpu.VMEM((2, 2 * 4 * ug, cg), BF16),
        pltpu.VMEM((2 * 4 * ud, cd), BF16),
        pltpu.VMEM((2, 2, 2, ug // 2, cg), BF16),
        pltpu.VMEM((2, 2, ud // 2, cd), BF16),
        pltpu.VMEM((2, 2, 2, ug, cg), BF16),
        pltpu.VMEM((2, 2, ud, cd), BF16),
        pltpu.VMEM((8, D), F32),
        pltpu.VMEM((2, 1, D), F32),
        pltpu.VMEM((4, 1, D), F32),
        pltpu.VMEM((16, 1, D), F32),
        dma((8,)),
        dma((20,)),
        dma((STEPS, 3)),
        dma((2, 2, 2)),
        dma((2, 2, 2)),
        dma((2,)),
        dma((STEPS,)),
        dma((14,)),
        dma((3, 4)),
        dma((6, 28)),
        dma((6, 28)),
        dma((19,)),
        dma((19,)),
    ]
    return pl.pallas_call(
        kernel,
        name="fused",
        out_shape=(
            pltpu.VMEM((ROWS, D), BF16),
            pltpu.VMEM((1, D), F32),
            pltpu.VMEM((D, FF), BF16),
            pltpu.VMEM((D, FF), BF16),
            pltpu.VMEM((FF, D), BF16),
        ),
        in_specs=[any_space] * 6,
        out_specs=(vmem,) * 5,
        scratch_shapes=scratch,
        compiler_params=pltpu.CompilerParams(
            collective_id=0, has_side_effects=True, vmem_limit_bytes=60_800_000
        ),
    )(tokens_in, norm_gain.reshape(1, D), gate_weight, up_weight, down_weight, out_grad)


def scaled(factor, ga, up, dn, gin, gain, ga_out, up_out, dn_out, gin_out, gain_out, fa, fu, fd, sems):
    copies = [
        pltpu.make_async_copy(gin, gin_out, sems.at[0]),
        pltpu.make_async_copy(gain, gain_out, sems.at[1]),
    ]
    for c in copies:
        c.start()

    def piece(i, src, mid, out, start, size, step, scale):
        def convert(r):
            rows = pl.ds(start + r, step)
            mid[rows, :] = src[rows, :].astype(F32) * scale

        over(size, step, convert)
        rows = pl.ds(start, size)
        copies.append(pltpu.make_async_copy(mid.at[rows], out.at[rows], sems.at[i]))
        copies[-1].start()

    for n in range(4):
        piece(2 + n, ga, fa, ga_out, n * 512, 512, 64, factor)
        piece(6 + n, up, fu, up_out, n * 512, 512, 64, factor)
    for n in range(4):
        piece(10 + n, dn, fd, dn_out, n * 96, 96, 16, 0.5 * factor)
    for c in copies:
        c.wait()


def shards(tokens_in, norm_gain, gate_weight, up_weight, down_weight, out_grad):
    row_count = tokens_in.shape[0]
    total_tokens = row_count * lax.axis_size("rep") * lax.axis_size("fs") * lax.axis_size("tp")
    factor = float(total_tokens) ** (-0.5)
    grad_in, gain_row, ga, up, dn = fused(tokens_in, norm_gain, gate_weight, up_weight, down_weight, out_grad)
    shapes = ((D, FF), (D, FF), (FF, D))
    grad_gate, grad_up, grad_down, grad_in, gain_row = pl.pallas_call(
        functools.partial(scaled, factor),
        name="scaled",
        out_shape=(
            *(jax.ShapeDtypeStruct(shape, F32) for shape in shapes),
            jax.ShapeDtypeStruct((ROWS, D), BF16),
            jax.ShapeDtypeStruct((1, D), F32),
        ),
        in_specs=[pl.BlockSpec(memory_space=pltpu.VMEM)] * 5,
        out_specs=(pl.BlockSpec(memory_space=pl.ANY),) * 5,
        scratch_shapes=[*(pltpu.VMEM(shape, F32) for shape in shapes), pltpu.SemaphoreType.DMA((14,))],
        compiler_params=pltpu.CompilerParams(vmem_limit_bytes=30_000_000),
    )(*(pltpu.with_memory_space_constraint(v, pltpu.VMEM) for v in (ga, up, dn, grad_in, gain_row)))
    grad_gain = gain_row.reshape(D)
    return (grad_in, grad_gain, grad_gate, grad_up, grad_down)


def solution(mesh):
    in_specs = (
        P(("rep", "fs", "tp"), None),
        P(),
        P(None, ("fs", "tp")),
        P(None, ("fs", "tp")),
        P(("fs", "tp"), None),
        P(("rep", "fs", "tp"), None),
    )
    out_specs = (
        P(("rep", "fs", "tp"), None),
        P(),
        P(None, ("fs", "tp")),
        P(None, ("fs", "tp")),
        P(("fs", "tp"), None),
    )
    return jax.shard_map(shards, mesh=mesh, in_specs=in_specs, out_specs=out_specs, check_vma=False)
```

```python
import functools

import jax
import jax.numpy as jnp
from jax import lax
from jax.experimental import pallas as pl
from jax.experimental.pallas import tpu as pltpu
from jax.sharding import PartitionSpec as P

norm_eps = 1e-06
MESH = pl.DeviceIdType.MESH
scope = jax.named_scope
F32 = jnp.float32
BF16 = jnp.bfloat16

D = 2048
FF = 384
ROWS = 256
PIECE = 64
HALF = 128
STEPS = 8
CH = 256
WIDE = 512
UNITS = (64, 64, 96)
WIDTHS = (FF, FF, CH)


def over(n, step, body):
    def go(i, carry):
        body(pl.multiple_of(i * step, step))
        return carry

    lax.fori_loop(0, n // step, go, 0)


def dot(a, b, ca, cb):
    return lax.dot_general(a, b, (((ca,), (cb,)), ((), ())), preferred_element_type=F32)


def kernel(
    x_in, gain_in, gate_in, up_in, down_in, g_in,
    gin_out, gain_out, ga_out, up_out, dn_out,
    xg, wg, wdn, wgu_t, gain, acc_gu, acc_dn, pre, gh, dgu, hid,
    kept, away, from_sib, far_l, far_r, near_l, near_r,
    wd, s1g, s1d, t1g, t1d, vg, vd, s2g, s2d, t2g, t2d,
    g_acc, g_tp, g_y, g_rep,
    ld_sem, ag_send, ag_recv, ag7_recv, sib_send, sib_recv, rs_send, rs_recv,
    ar_send, ar_recv, gn_send, gn_recv,
):
    rep, fs, tp = lax.axis_index("rep"), lax.axis_index("fs"), lax.axis_index("tp")
    z, x = rep // 4, rep % 4

    def y_at(k):
        return {"rep": rep, "fs": (fs + k) % 4, "tp": tp}

    def x_at(k):
        return {"rep": z * 4 + (x + k) % 4, "fs": fs, "tp": tp}

    def z_at(k):
        return {"rep": ((z + k) % 4) * 4 + x, "fs": fs, "tp": tp}

    sib = {"rep": rep, "fs": fs, "tp": 1 - tp}

    def remote(src, dst, send, recv, to):
        return pltpu.make_async_remote_copy(
            src_ref=src, dst_ref=dst, send_sem=send, recv_sem=recv, device_id=to, device_id_type=MESH
        )

    def taken(ref, sem):
        pltpu.make_async_copy(ref, ref, sem).wait()

    loads = []
    for s in range(2):
        loads.append(pltpu.make_async_copy(x_in.at[pl.ds(s * HALF, HALF)], away.at[s], ld_sem.at[2 * s]))
        loads.append(pltpu.make_async_copy(g_in.at[pl.ds(s * HALF, HALF)], xg.at[s, 1, pl.ds(0, HALF)], ld_sem.at[2 * s + 1]))
    loads.append(pltpu.make_async_copy(gate_in, wg.at[0], ld_sem.at[4]))
    loads.append(pltpu.make_async_copy(up_in, wg.at[1], ld_sem.at[5]))
    loads.append(pltpu.make_async_copy(down_in, wdn, ld_sem.at[6]))
    loads.append(pltpu.make_async_copy(gain_in, gain, ld_sem.at[7]))
    for i in (7, 0, 1, 2, 3):
        loads[i].start()

    barrier = pltpu.get_barrier_semaphore()
    plane = [
        {"rep": ((z + k // 4) % 4) * 4 + (x + k % 4) % 4, "fs": fs, "tp": tp} for k in range(1, 16)
    ]
    partners = [sib] + [y_at(k) for k in (1, 3, 2)] + plane
    for p in partners:
        pl.semaphore_signal(barrier, inc=1, device_id=p, device_id_type=MESH)

    def to_sib(s):
        return remote(
            xg.at[s, :, pl.ds(0, HALF)], xg.at[s, :, pl.ds(HALF, HALF)], ag_send, ag_recv.at[s, 1], sib
        )

    def own_piece(p, j):
        src = xg.at[p // 2, :, pl.ds((p % 2) * PIECE, PIECE)]
        dst = xg.at[2 + p, :, pl.ds(j * PIECE, PIECE)]
        return remote(src, dst, ag_send, ag_recv.at[2 + p, 0], y_at(1 if j == 0 else 3))

    def onward(s, j):
        return remote(
            xg.at[s, :, pl.ds(j * PIECE, PIECE)],
            xg.at[s + 4 - 2 * j, :, pl.ds(j * PIECE, PIECE)],
            ag_send,
            ag_recv.at[s + 4 - 2 * j, 0],
            y_at(1 if j == 0 else 3),
        )

    def last_onward(j, q):
        rows = pl.ds(j * PIECE, PIECE)
        return remote(
            xg.at[3 + 2 * j, q, rows], xg.at[7, q, rows], ag_send, ag7_recv.at[0, q], y_at(1 if j == 0 else 3)
        )

    def last_to_sib(j, q):
        near, far = pl.ds(j * PIECE, PIECE), pl.ds(HALF + j * PIECE, PIECE)
        return remote(xg.at[7, q, near], xg.at[7, q, far], ag_send, ag7_recv.at[1, q], sib)

    def last_pass(q):
        taken(xg.at[7, q, pl.ds(0, HALF)], ag7_recv.at[0, q])
        for j in range(2):
            last_to_sib(j, q).start()

    def last_in(q):
        taken(xg.at[7, q, pl.ds(HALF, HALF)], ag7_recv.at[1, q])

    def arrival(s):
        taken(xg.at[s, :, pl.ds(0, HALF)], ag_recv.at[s, 0])

    def norm(p):
        def rows16(i, carry):
            rows = pl.ds(pl.multiple_of((p % 2) * PIECE + i * 16, 16), 16)
            floats = away[p // 2, rows, :].astype(F32)
            inverse = lax.rsqrt(jnp.mean(floats * floats, axis=-1, keepdims=True) + norm_eps)
            xg[p // 2, 0, rows, :] = (floats * inverse * gain[...]).astype(BF16)
            return carry

        lax.fori_loop(0, PIECE // 16, rows16, 0, unroll=2)

    def leave(p):
        own_piece(p, 0).start()
        own_piece(p, 1).start()

    with scope("first"):
        loads[7].wait()
        loads[0].wait()
        loads[1].wait()
        for c in loads[4:7]:
            c.start()
        norm(0)
    with scope("barrier"):
        pl.semaphore_wait(barrier, len(partners))
    leave(0)
    norm(1)
    loads[2].wait()
    norm(2)
    to_sib(0).start()
    leave(1)
    norm(3)
    loads[3].wait()
    leave(2)
    for c in loads[4:7]:
        c.wait()
    to_sib(1).start()
    leave(3)

    def turn(c):
        cols = pl.ds(c, CH)
        wgu_t[:FF, cols] = wg[0, cols, :].T
        wgu_t[FF:, cols] = wg[1, cols, :].T

    with scope("turn"):
        over(D, CH, turn)

    def zero(r):
        acc_gu[pl.ds(r, 64), :] = jnp.zeros((64, 2 * FF), F32)
        acc_dn[pl.ds(pl.multiple_of(r // 64 * 96, 96), 96), :] = jnp.zeros((96, CH), F32)

    with scope('zero'):
        over(D, 64, zero)

    def sib_sum(s):
        return remote(away.at[s % 2], from_sib.at[s], sib_send.at[s % 2], sib_recv.at[s], sib)

    def chip_sum(s):
        sib_sum(s).wait_recv()

        def add(r):
            rows = pl.ds(r, 32)
            kept[s, rows, :] = (kept[s, rows, :].astype(F32) + from_sib[s, rows, :].astype(F32)).astype(BF16)

        over(HALF, 32, add)

    def early_right(q):
        return remote(kept.at[q, pl.ds(PIECE, PIECE)], near_l.at[q - 2], rs_send, rs_recv.at[2], y_at(1))

    def early_left(q):
        return remote(kept.at[q, pl.ds(0, PIECE)], near_r.at[q - 2], rs_send, rs_recv.at[2], y_at(3))

    def far_left(q):
        return remote(kept.at[q, pl.ds(0, PIECE)], far_r.at[q - 6], rs_send, rs_recv.at[q - 6], y_at(3))

    def far_right(q):
        return remote(kept.at[q, pl.ds(PIECE, PIECE)], far_l.at[q - 6], rs_send, rs_recv.at[q - 6], y_at(1))

    def late_left(q):
        return remote(kept.at[q, pl.ds(0, PIECE)], near_r.at[q - 2], rs_send, rs_recv.at[2], y_at(3))

    def late_right(q):
        return remote(kept.at[q, pl.ds(PIECE, PIECE)], near_l.at[q - 2], rs_send, rs_recv.at[2], y_at(1))

    packed = [(*(ref.at[k] for ref in (wg, s1g, t1g, vg, s2g, t2g)), out) for k, out in enumerate((ga_out, up_out))]
    packed.append((wd, s1d, t1d, vd, s2d, t2d, dn_out))
    halves = ((x, z, x_at, z_at), (z, x, z_at, x_at))
    streams = [(h, k) for k in range(3) for h in range(2)]

    class Ring:
        def __init__(self, h, k, src, base, size, mid, end, index, at, sem):
            self.src, self.size, self.mid, self.end = src, size, mid, end
            half = size // 2
            self.half = half
            f = h * 3 + k

            def rows(chunk, part):
                start = base + ((index + chunk) % 4) * size + part * half
                return pl.ds(pl.multiple_of(start, 16), half)

            self.rows = rows

            def copy(i, chunk, part, dst, to):
                return remote(src.at[rows(chunk, part)], dst, ar_send.at[f, sem], ar_recv.at[f, 2 * sem + i], at(to))

            self.sems = ar_send.at[f, sem], ar_recv.at[f, 2 * sem], ar_recv.at[f, 2 * sem + 1]
            self.bytes = lambda n: packed[k][0].at[pl.ds(0, n)]

            self.first = [
                copy(0, 2, 0, mid.at[h, 1], 3),
                copy(0, 2, 1, mid.at[h, 0], 1),
                copy(1, 3, 1, end.at[h, 1, pl.ds(half, half)], 3),
                copy(1, 1, 0, end.at[h, 0, pl.ds(0, half)], 1),
            ]
            self.second = [
                copy(1, 3, 0, end.at[h, 1, pl.ds(0, half)], 3),
                copy(1, 1, 1, end.at[h, 0, pl.ds(half, half)], 1),
            ]
            self.h = h

        def mid_out(self):
            for c in self.first[:2]:
                c.start()

        def end_out(self):
            for c in self.first[2:]:
                c.start()

        def relay(self):
            h = self.h
            taken(self.bytes(self.size), self.sems[1])
            for i, (chunk, part, side) in enumerate(((3, 0, 1), (1, 1, 0))):
                rows = self.rows(chunk, part)
                self.src[rows, :] = (self.src[rows, :].astype(F32) + self.mid[h, side].astype(F32)).astype(BF16)
                self.second[i].start()

        def finish(self, store):
            h = self.h
            taken(self.bytes(2 * self.size), self.sems[2])
            for part in range(2):
                local = pl.ds(part * self.half, self.half)
                total = self.src[self.rows(0, part), :].astype(F32)
                total = total + self.end[h, 0, local, :].astype(F32) + self.end[h, 1, local, :].astype(F32)
                store(part, total.astype(BF16))

        def drain(self):
            taken(self.bytes(3 * self.size), self.sems[0])

    rings1, rings2 = {}, {}
    for h, k in streams:
        w, s1, t1, v, s2, t2, out = packed[k]
        i1, i2, at1, at2 = halves[h]
        unit = UNITS[k]
        rings1[h, k] = Ring(h, k, w, h * 16 * unit, 4 * unit, s1, t1, i1, at1, 0)
        rings2[h, k] = Ring(h, k, v, h * 4 * unit, unit, s2, t2, i2, at2, 1)

    def step(s, carry):
        with scope("w_sib"):

            @pl.when(s < STEPS - 1)
            def _():
                to_sib(s).wait_recv()

            @pl.when(s == STEPS - 1)
            def _():
                last_in(0)

        with scope("pre"):
            pre[:, :FF] = dot(xg[s, 0], wg[0], 1, 0)
            pre[:, FF:] = dot(xg[s, 0], wg[1], 1, 0)

        @pl.when(s == STEPS - 1)
        def _():
            with scope("w_last"):
                last_pass(1)
                last_in(1)

        with scope("gh"):
            gh[...] = dot(xg[s, 1], wdn[...], 1, 1)

        def gates(r):
            rows = pl.ds(r, 32)
            gate_pre, up_pre = pre[rows, :FF], pre[rows, FF:]
            grad_hidden = 0.5 * gh[rows, :]
            sigma = jax.nn.sigmoid(gate_pre)
            active = gate_pre * sigma
            hid[rows, :] = (active * up_pre).astype(BF16)
            dgu[rows, :FF] = (grad_hidden * up_pre * sigma * (1.0 + gate_pre * (1.0 - sigma))).astype(BF16)
            dgu[rows, FF:] = (grad_hidden * active).astype(BF16)

        with scope("gates"):
            over(ROWS, 32, gates)

        def part_gu(c, width):
            cols = pl.ds(pl.multiple_of(c, width), width)
            return cols, acc_gu[cols, :] + dot(xg[s, 0, :, cols], dgu[...], 0, 0)

        def part_dn(c, store):
            value = dot(hid[...], xg[s, 1, :, pl.ds(c, WIDE)], 0, 0)
            for i in range(WIDE // CH):
                rows = pl.ds(pl.multiple_of((c // CH + i) * FF, FF), FF)
                store(rows, acc_dn[rows, :] + value[:, i * CH : (i + 1) * CH])

        @pl.when(s < STEPS - 1)
        def _():
            def keep_dn(rows, value):
                acc_dn[rows, :] = value

            def weights(c):
                cols, value = part_gu(c, WIDE)
                acc_gu[cols, :] = value
                part_dn(c, keep_dn)

            with scope("weights"):
                over(D, WIDE, weights)

        @pl.when(s == STEPS - 1)
        def _():
            def last_gu(c):
                cols, value = part_gu(c, CH)
                wg[0, cols, :] = value[:, :FF].astype(BF16)
                wg[1, cols, :] = value[:, FF:].astype(BF16)

            def last_dn(rows, value):
                wd[rows, :] = value.astype(BF16)

            for n in (2, 3, 1, 0):
                with scope("last_gu"):
                    for h in range(2):
                        last_gu((h * 4 + (halves[h][0] + n) % 4) * CH)
                for h in range(2):
                    if n == 2:
                        rings1[h, 0].mid_out()
                        rings1[h, 1].mid_out()
                    if n == 1:
                        rings1[h, 0].end_out()
            with scope("last_dn"):
                over(D, WIDE, lambda c: part_dn(c, last_dn))

        @pl.when((s >= 1) & (s < STEPS - 2))
        def _():
            with scope("w_nbr"):
                arrival(s + 1)
            to_sib(s + 1).start()

        @pl.when(s == STEPS - 2)
        def _():
            with scope("w_nbr"):
                last_pass(0)

        @pl.when(s == 1)
        def _():
            onward(s + 1, 0).start()

        @pl.when(s == 3)
        def _():
            onward(s + 1, 1).start()

        @pl.when(s == 2)
        def _():
            for q in range(2):
                last_onward(0, q).start()

        @pl.when(s == 4)
        def _():
            for q in range(2):
                last_onward(1, q).start()

        @pl.when(s >= 2)
        def _():
            sib_sum(s).wait_send()

        def terms(c):
            cols = pl.ds(c, WIDE)
            term = dot(dgu[...], wgu_t[:, cols], 1, 0).astype(BF16)
            kept[s, :, cols] = term[:HALF]
            away[s % 2, :, cols] = term[HALF:]

        with scope("terms"):
            over(D, WIDE, terms)

        @pl.when(s >= 1)
        def _():
            with scope("chipsum"):
                chip_sum(s - 1)

        sib_sum(s).start()

        @pl.when((s == 3) | (s == 4))
        def _():
            early_right(s - 1).start()

        @pl.when((s == 5) | (s == 6))
        def _():
            early_left(s - 1).start()

        return carry

    lax.fori_loop(0, STEPS, step, 0)

    def add_far(q, lo, far):
        def add(r):
            rows = pl.ds(lo + r, 32)
            kept[q, rows, :] = (kept[q, rows, :].astype(F32) + far[pl.ds(r, 32), :].astype(F32)).astype(BF16)

        over(PIECE, 32, add)

    def store_v(h, k):
        v, unit = packed[k][3], UNITS[k]

        def store(part, value):
            v[pl.ds(h * 4 * unit + part * 2 * unit, 2 * unit), :] = value

        return store

    class Back:
        def __init__(self, h, k):
            i1, i2, at1, at2 = halves[h]
            out, f, unit = packed[k][6], h * 3 + k, UNITS[k]
            half = unit // 2

            def spot(ra, rb, part=None):
                a, b = (i1 + ra) % 4, (i2 + rb) % 4
                rows = half if part is not None else unit
                if k < 2:
                    start = ((h * 4 + a) * 4 + b) * unit + (part or 0) * half
                    return pl.ds(pl.multiple_of(start, 16), rows), slice(None)
                start = b * unit + (part or 0) * half
                return pl.ds(pl.multiple_of(start, 16), rows), pl.ds(pl.multiple_of((h * 4 + a) * CH, CH), CH)

            def copy(i, to, *where):
                view = out.at[spot(*where)]
                return remote(view, view, ar_send.at[f, 2], ar_recv.at[f, 4 + i], to)

            self.taken = lambda units, sem: taken(packed[k][0].at[pl.ds(0, units * unit)], sem)
            self.sems = ar_send.at[f, 2], [ar_recv.at[f, 4 + i] for i in range(6)]

            self.out, self.spot = out, spot
            self.own2 = [copy(0, at2(1), 0, 0), copy(0, at2(3), 0, 0)]
            self.on2 = [copy(1, at2(1), 0, 3, 0), copy(1, at2(3), 0, 1, 1)]
            rightward, leftward = (2, 5, 5, 3), (5, 3, 4, 5)
            self.out1 = [
                [copy(rightward[r], at1(1), 0, r), copy(leftward[r], at1(3), 0, r)] for r in range(4)
            ]
            self.on1 = {
                0: copy(5, at1(1), 3, 0),
                3: copy(5, at1(1), 3, 3),
                1: copy(5, at1(3), 1, 1),
                2: copy(5, at1(3), 1, 2),
            }

        def store(self, part, value):
            self.out[self.spot(0, 0, part)] = value

        def send(self, r):
            for c in self.out1[r]:
                c.start()

        def begin(self):
            for c in self.own2:
                c.start()
            self.send(0)

        def middle(self):
            self.taken(2, self.sems[1][0])
            for on, r in zip(self.on2, (3, 1)):
                on.start()
                self.send(r)

        def last(self):
            self.taken(1, self.sems[1][1])
            self.send(2)

        def pass_on(self, *which):
            self.taken(len(which), self.sems[1][{0: 2, 3: 3, 2: 4}[which[0]]])
            for r in which:
                self.on1[r].start()

        def finish(self):
            self.taken(8, self.sems[1][5])

        def drain(self):
            self.taken(15, self.sems[0])

    back = {(h, k): Back(h, k) for h, k in streams}

    def own_rows(i, carry):
        r = pl.multiple_of(i * 16, 16)
        s, p = i // 8, i // 4
        half, piece = pl.ds(pl.multiple_of((i % 8) * 16, 16), 16), pl.ds(pl.multiple_of((i % 4) * 16, 16), 16)
        grad = kept[s, half, :].astype(F32) + near_l[p, piece, :].astype(F32) + near_r[p, piece, :].astype(F32)
        floats = away[s, half, :].astype(F32)
        inverse = lax.rsqrt(jnp.mean(floats * floats, axis=-1, keepdims=True) + norm_eps)
        unit_rows = floats * inverse
        gained = grad * unit_rows
        g_acc[...] += gained[:8] + gained[8:]
        scaled = grad * gain[...]
        mean = jnp.mean(scaled * unit_rows, axis=-1, keepdims=True)
        result = xg[s, 1, half, :].astype(F32) + inverse * scaled - unit_rows * inverse * mean
        gin_out[pl.ds(r, 16), :] = result.astype(BF16)
        return carry


    def spread(buffer, index, targets, group):
        for to in targets:
            remote(buffer.at[index], buffer.at[index], gn_send.at[group], gn_recv.at[group], to).start()

    def gathered(buffer, count, group):
        for sems in (gn_recv, gn_send):
            taken(buffer.at[pl.ds(0, count)], sems.at[group])

    def both(k, act):
        for h in range(2):
            act(h, k)

    def relay1(h, k):
        rings1[h, k].relay()

    def finish1(h, k):
        rings1[h, k].finish(store_v(h, k))
        rings2[h, k].mid_out()
        rings2[h, k].end_out()

    def relay2(h, k):
        rings2[h, k].relay()

    def finish2(h, k):
        rings2[h, k].finish(back[h, k].store)
        back[h, k].begin()

    def near2(h, k):
        back[h, k].middle()

    def far2(h, k):
        back[h, k].last()

    def pass0(h, k):
        back[h, k].pass_on(0)

    def pass1(h, k):
        back[h, k].pass_on(3, 1)

    def pass2(h, k):
        back[h, k].pass_on(2)

    def far1(h, k):
        back[h, k].finish()

    def run(name, k, act):
        with scope(f"{name}{k}"):
            both(k, act)

    far_left(6).start()
    far_right(6).start()
    with scope("chip7"):
        chip_sum(7)
    far_left(7).start()
    far_right(7).start()
    sib_sum(6).wait_send()
    sib_sum(7).wait_send()
    again = [pltpu.make_async_copy(x_in.at[pl.ds(s * HALF, HALF)], away.at[s], ld_sem.at[s]) for s in range(2)]
    for c in again:
        c.start()

    def far(i):
        with scope("far"):
            taken(kept.at[0], rs_recv.at[i])
            add_far(2 + i, 0, far_r.at[i])
            late_left(2 + i).start()
            add_far(4 + i, PIECE, far_l.at[i])
            late_right(4 + i).start()

    def drain_gather():
        taken(xg.at[pl.ds(0, 7)], ag_send)

    def drain_tokens():
        taken(kept.at[pl.ds(0, 6)], rs_send)

    def drain_rings(rings, k):
        both(k, lambda h, k: rings[h, k].drain())

    def drain_out(k):
        both(k, lambda h, k: back[h, k].drain())

    run("relay1", 0, relay1)
    run("relay1", 1, relay1)
    both(2, lambda h, k: rings1[h, k].mid_out())
    run("finish1", 0, finish1)
    both(1, lambda h, k: rings1[h, k].end_out())
    both(2, lambda h, k: rings1[h, k].end_out())
    far(0)
    drain_gather()
    run("relay2", 0, relay2)
    run("relay1", 2, relay1)
    run("finish1", 1, finish1)
    far(1)
    drain_rings(rings1, 0)
    drain_rings(rings1, 1)
    run("finish2", 0, finish2)
    run("finish1", 2, finish1)
    run("relay2", 1, relay2)
    run("near2", 0, near2)
    run("relay2", 2, relay2)
    run("finish2", 1, finish2)
    run("far2", 0, far2)
    run("pass1", 0, pass1)
    run("finish2", 2, finish2)
    with scope("w_rs"):
        for c in again:
            c.wait()
        taken(kept.at[pl.ds(0, 4)], rs_recv.at[2])
    with scope("own"):
        g_acc[...] = jnp.zeros((8, D), F32)
        lax.fori_loop(0, ROWS // 16, own_rows, 0, unroll=2)
        g_tp[tp] = jnp.sum(g_acc[...], axis=0, keepdims=True)
    spread(g_tp, tp, [sib], 0)
    run("near2", 1, near2)
    drain_rings(rings1, 2)
    drain_tokens()
    run("near2", 2, near2)
    with scope("g1"):
        gathered(g_tp, 1, 0)
        g_y[fs] = g_tp[0] + g_tp[1]
        spread(g_y, fs, [y_at(1), y_at(2), y_at(3)], 1)
    run("pass2", 0, pass2)
    drain_rings(rings2, 0)
    run("far2", 1, far2)
    drain_rings(rings2, 1)
    drain_rings(rings2, 2)
    run("far2", 2, far2)
    with scope("g2"):
        gathered(g_y, 3, 1)
        g_rep[rep] = (g_y[0] + g_y[1]) + (g_y[2] + g_y[3])
        spread(g_rep, rep, plane, 2)
    run("pass0", 0, pass0)
    run("pass0", 1, pass0)
    run("pass1", 1, pass1)
    run("pass1", 2, pass1)
    run("pass2", 1, pass2)
    run("pass2", 2, pass2)
    run("pass0", 2, pass0)
    with scope("g3"):
        gathered(g_rep, 15, 2)
        total = g_rep[0]
        for i in range(1, 16):
            total = total + g_rep[i]
        gain_out[...] = total
    run("far1", 0, far1)
    run("far1", 1, far1)
    run("far1", 2, far1)

    for k in range(3):
        drain_out(k)


def fused(tokens_in, norm_gain, gate_weight, up_weight, down_weight, out_grad):
    any_space = pl.BlockSpec(memory_space=pl.ANY)
    vmem = pl.BlockSpec(memory_space=pltpu.VMEM)
    (ug, _, ud), (cg, _, cd) = UNITS, WIDTHS
    dma = pltpu.SemaphoreType.DMA
    scratch = [
        pltpu.VMEM((STEPS, 2, ROWS, D), BF16),
        pltpu.VMEM((2, D, FF), BF16),
        pltpu.VMEM((FF, D), BF16),
        pltpu.VMEM((2 * FF, D), BF16),
        pltpu.VMEM((1, D), F32),
        pltpu.VMEM((D, 2 * FF), F32),
        pltpu.VMEM((8 * FF, CH), F32),
        pltpu.VMEM((ROWS, 2 * FF), F32),
        pltpu.VMEM((ROWS, FF), F32),
        pltpu.VMEM((ROWS, 2 * FF), BF16),
        pltpu.VMEM((ROWS, FF), BF16),
        pltpu.VMEM((STEPS, HALF, D), BF16),
        pltpu.VMEM((2, HALF, D), BF16),
        pltpu.VMEM((STEPS, HALF, D), BF16),
        pltpu.VMEM((2, PIECE, D), BF16),
        pltpu.VMEM((2, PIECE, D), BF16),
        pltpu.VMEM((4, PIECE, D), BF16),
        pltpu.VMEM((4, PIECE, D), BF16),
        pltpu.VMEM((8 * FF, cd), BF16),
        pltpu.VMEM((2, 2, 2, 2 * ug, cg), BF16),
        pltpu.VMEM((2, 2, 2 * ud, cd), BF16),
        pltpu.VMEM((2, 2, 2, 4 * ug, cg), BF16),
        pltpu.VMEM((2, 2, 4 * ud, cd), BF16),
        pltpu.VMEM((2, 2 * 4 * ug, cg), BF16),
        pltpu.VMEM((2 * 4 * ud, cd), BF16),
        pltpu.VMEM((2, 2, 2, ug // 2, cg), BF16),
        pltpu.VMEM((2, 2, ud // 2, cd), BF16),
        pltpu.VMEM((2, 2, 2, ug, cg), BF16),
        pltpu.VMEM((2, 2, ud, cd), BF16),
        pltpu.VMEM((8, D), F32),
        pltpu.VMEM((2, 1, D), F32),
        pltpu.VMEM((4, 1, D), F32),
        pltpu.VMEM((16, 1, D), F32),
        dma((8,)),
        dma,
        dma((STEPS, 2)),
        dma((2, 2)),
        dma((2,)),
        dma((STEPS,)),
        dma,
        dma((3,)),
        dma((6, 3)),
        dma((6, 10)),
        dma((3,)),
        dma((3,)),
    ]
    return pl.pallas_call(
        kernel,
        name="fused",
        out_shape=(
            pltpu.VMEM((ROWS, D), BF16),
            pltpu.VMEM((1, D), F32),
            pltpu.VMEM((D, FF), BF16),
            pltpu.VMEM((D, FF), BF16),
            pltpu.VMEM((FF, D), BF16),
        ),
        in_specs=[any_space] * 6,
        out_specs=(vmem,) * 5,
        scratch_shapes=scratch,
        compiler_params=pltpu.CompilerParams(
            collective_id=0, has_side_effects=True, vmem_limit_bytes=60_800_000
        ),
    )(tokens_in, norm_gain.reshape(1, D), gate_weight, up_weight, down_weight, out_grad)


def scaled(factor, ga, up, dn, gin, gain, ga_out, up_out, dn_out, gin_out, gain_out, fa, fu, fd, sems):
    copies = [
        pltpu.make_async_copy(gin, gin_out, sems.at[0]),
        pltpu.make_async_copy(gain, gain_out, sems.at[1]),
    ]
    for c in copies:
        c.start()

    def piece(i, src, mid, out, start, size, step, scale):
        def convert(r):
            rows = pl.ds(start + r, step)
            mid[rows, :] = src[rows, :].astype(F32) * scale

        over(size, step, convert)
        rows = pl.ds(start, size)
        copies.append(pltpu.make_async_copy(mid.at[rows], out.at[rows], sems.at[i]))
        copies[-1].start()

    for n in range(4):
        piece(2 + n, ga, fa, ga_out, n * 512, 512, 64, factor)
        piece(6 + n, up, fu, up_out, n * 512, 512, 64, factor)
    for n in range(4):
        piece(10 + n, dn, fd, dn_out, n * 96, 96, 16, 0.5 * factor)
    for c in copies:
        c.wait()


def shards(tokens_in, norm_gain, gate_weight, up_weight, down_weight, out_grad):
    row_count = tokens_in.shape[0]
    total_tokens = row_count * lax.axis_size("rep") * lax.axis_size("fs") * lax.axis_size("tp")
    factor = float(total_tokens) ** (-0.5)
    grad_in, gain_row, ga, up, dn = fused(tokens_in, norm_gain, gate_weight, up_weight, down_weight, out_grad)
    shapes = ((D, FF), (D, FF), (FF, D))
    grad_gate, grad_up, grad_down, grad_in, gain_row = pl.pallas_call(
        functools.partial(scaled, factor),
        name="scaled",
        out_shape=(
            *(jax.ShapeDtypeStruct(shape, F32) for shape in shapes),
            jax.ShapeDtypeStruct((ROWS, D), BF16),
            jax.ShapeDtypeStruct((1, D), F32),
        ),
        in_specs=[pl.BlockSpec(memory_space=pltpu.VMEM)] * 5,
        out_specs=(pl.BlockSpec(memory_space=pl.ANY),) * 5,
        scratch_shapes=[*(pltpu.VMEM(shape, F32) for shape in shapes), pltpu.SemaphoreType.DMA((14,))],
        compiler_params=pltpu.CompilerParams(vmem_limit_bytes=30_000_000),
    )(*(pltpu.with_memory_space_constraint(v, pltpu.VMEM) for v in (ga, up, dn, grad_in, gain_row)))
    grad_gain = gain_row.reshape(D)
    return (grad_in, grad_gain, grad_gate, grad_up, grad_down)


def solution(mesh):
    in_specs = (
        P(("rep", "fs", "tp"), None),
        P(),
        P(None, ("fs", "tp")),
        P(None, ("fs", "tp")),
        P(("fs", "tp"), None),
        P(("rep", "fs", "tp"), None),
    )
    out_specs = (
        P(("rep", "fs", "tp"), None),
        P(),
        P(None, ("fs", "tp")),
        P(None, ("fs", "tp")),
        P(("fs", "tp"), None),
    )
    return jax.shard_map(shards, mesh=mesh, in_specs=in_specs, out_specs=out_specs, check_vma=False)
```

```python
import functools

import jax
import jax.numpy as jnp
from jax import lax
from jax.experimental import pallas as pl
from jax.experimental.pallas import tpu as pltpu
from jax.sharding import PartitionSpec as P

norm_eps = 1e-06
MESH = pl.DeviceIdType.MESH
scope = jax.named_scope
F32 = jnp.float32
BF16 = jnp.bfloat16

D = 2048
FF = 384
ROWS = 256
PIECE = 64
HALF = 128
STEPS = 8
CH = 256
WIDE = 512
UNITS = (64, 64, 96)
WIDTHS = (FF, FF, CH)


def over(n, step, body):
    def go(i, carry):
        body(pl.multiple_of(i * step, step))
        return carry

    lax.fori_loop(0, n // step, go, 0)


def dot(a, b, ca, cb):
    return lax.dot_general(a, b, (((ca,), (cb,)), ((), ())), preferred_element_type=F32)


def kernel(
    x_in, gain_in, gate_in, up_in, down_in, g_in,
    gin_out, gain_out, ga_out, up_out, dn_out,
    xg, wg, wdn, wgu_t, gain, acc_gu, acc_dn, pre, gh, dgu, hid,
    kept, away, from_sib, far_l, far_r, near_l, near_r,
    wd, s1g, s1d, t1g, t1d, vg, vd, s2g, s2d, t2g, t2d,
    g_acc, g_tp, g_y, g_rep,
    ld_sem, ag_send, ag_recv, ag7_recv, sib_send, sib_recv, rs_send, rs_recv,
    ar_send, ar_recv, gn_send, gn_recv,
):
    rep, fs, tp = lax.axis_index("rep"), lax.axis_index("fs"), lax.axis_index("tp")
    z, x = rep // 4, rep % 4

    def y_at(k):
        return {"rep": rep, "fs": (fs + k) % 4, "tp": tp}

    def x_at(k):
        return {"rep": z * 4 + (x + k) % 4, "fs": fs, "tp": tp}

    def z_at(k):
        return {"rep": ((z + k) % 4) * 4 + x, "fs": fs, "tp": tp}

    sib = {"rep": rep, "fs": fs, "tp": 1 - tp}

    def remote(src, dst, send, recv, to):
        return pltpu.make_async_remote_copy(
            src_ref=src, dst_ref=dst, send_sem=send, recv_sem=recv, device_id=to, device_id_type=MESH
        )

    def taken(ref, sem):
        pltpu.make_async_copy(ref, ref, sem).wait()

    loads = []
    for s in range(2):
        loads.append(pltpu.make_async_copy(x_in.at[pl.ds(s * HALF, HALF)], away.at[s], ld_sem.at[2 * s]))
        loads.append(pltpu.make_async_copy(g_in.at[pl.ds(s * HALF, HALF)], xg.at[s, 1, pl.ds(0, HALF)], ld_sem.at[2 * s + 1]))
    loads.append(pltpu.make_async_copy(gate_in, wg.at[0], ld_sem.at[4]))
    loads.append(pltpu.make_async_copy(up_in, wg.at[1], ld_sem.at[5]))
    loads.append(pltpu.make_async_copy(down_in, wdn, ld_sem.at[6]))
    loads.append(pltpu.make_async_copy(gain_in, gain, ld_sem.at[7]))
    for i in (7, 0, 1, 2, 3):
        loads[i].start()

    barrier = pltpu.get_barrier_semaphore()
    plane = [
        {"rep": ((z + k // 4) % 4) * 4 + (x + k % 4) % 4, "fs": fs, "tp": tp} for k in range(1, 16)
    ]
    partners = [sib] + [y_at(k) for k in (1, 3, 2)] + plane
    for p in partners:
        pl.semaphore_signal(barrier, inc=1, device_id=p, device_id_type=MESH)

    def to_sib(s):
        return remote(
            xg.at[s, :, pl.ds(0, HALF)], xg.at[s, :, pl.ds(HALF, HALF)], ag_send, ag_recv.at[s, 1], sib
        )

    def own_piece(p, j):
        src = xg.at[p // 2, :, pl.ds((p % 2) * PIECE, PIECE)]
        dst = xg.at[2 + p, :, pl.ds(j * PIECE, PIECE)]
        return remote(src, dst, ag_send, ag_recv.at[2 + p, 0], y_at(1 if j == 0 else 3))

    def onward(s, j):
        return remote(
            xg.at[s, :, pl.ds(j * PIECE, PIECE)],
            xg.at[s + 4 - 2 * j, :, pl.ds(j * PIECE, PIECE)],
            ag_send,
            ag_recv.at[s + 4 - 2 * j, 0],
            y_at(1 if j == 0 else 3),
        )

    parts = ((0, 0, PIECE), (1, 0, PIECE // 2), (1, PIECE // 2, PIECE // 2))

    def last_onward(j, q):
        plane, low, count = parts[q]
        rows = pl.ds(j * PIECE + low, count)
        return remote(
            xg.at[3 + 2 * j, plane, rows], xg.at[7, plane, rows], ag_send, ag7_recv.at[0, q], y_at(1 if j == 0 else 3)
        )

    def last_to_sib(j, q):
        plane, low, count = parts[q]
        near, far = pl.ds(j * PIECE + low, count), pl.ds(HALF + j * PIECE + low, count)
        return remote(xg.at[7, plane, near], xg.at[7, plane, far], ag_send, ag7_recv.at[1, q], sib)

    def last_pass(q):
        taken(xg.at[7, parts[q][0], pl.ds(0, 2 * parts[q][2])], ag7_recv.at[0, q])
        for j in range(2):
            last_to_sib(j, q).start()

    def last_in(q):
        taken(xg.at[7, parts[q][0], pl.ds(HALF, 2 * parts[q][2])], ag7_recv.at[1, q])

    def arrival(s):
        taken(xg.at[s, :, pl.ds(0, HALF)], ag_recv.at[s, 0])

    def norm(p):
        def rows16(i, carry):
            rows = pl.ds(pl.multiple_of((p % 2) * PIECE + i * 16, 16), 16)
            floats = away[p // 2, rows, :].astype(F32)
            inverse = lax.rsqrt(jnp.mean(floats * floats, axis=-1, keepdims=True) + norm_eps)
            xg[p // 2, 0, rows, :] = (floats * inverse * gain[...]).astype(BF16)
            return carry

        lax.fori_loop(0, PIECE // 16, rows16, 0, unroll=2)

    def leave(p):
        own_piece(p, 0).start()
        own_piece(p, 1).start()

    with scope("first"):
        loads[7].wait()
        loads[0].wait()
        loads[1].wait()
        for c in loads[4:7]:
            c.start()
        norm(0)
    with scope("barrier"):
        pl.semaphore_wait(barrier, len(partners))
    leave(0)
    norm(1)
    loads[2].wait()
    norm(2)
    to_sib(0).start()
    leave(1)
    norm(3)
    loads[3].wait()
    leave(2)
    for c in loads[4:7]:
        c.wait()
    to_sib(1).start()
    leave(3)

    def turn(c):
        cols = pl.ds(c, CH)
        wgu_t[:FF, cols] = wg[0, cols, :].T
        wgu_t[FF:, cols] = wg[1, cols, :].T

    with scope("turn"):
        over(D, CH, turn)

    def zero(r):
        acc_gu[pl.ds(r, 64), :] = jnp.zeros((64, 2 * FF), F32)
        acc_dn[pl.ds(pl.multiple_of(r // 64 * 96, 96), 96), :] = jnp.zeros((96, CH), F32)

    with scope('zero'):
        over(D, 64, zero)

    def sib_sum(s):
        return remote(away.at[s % 2], from_sib.at[s], sib_send.at[s % 2], sib_recv.at[s], sib)

    def chip_sum(s):
        sib_sum(s).wait_recv()

        def add(r):
            rows = pl.ds(r, 32)
            kept[s, rows, :] = (kept[s, rows, :].astype(F32) + from_sib[s, rows, :].astype(F32)).astype(BF16)

        over(HALF, 32, add)

    def early_right(q):
        return remote(kept.at[q, pl.ds(PIECE, PIECE)], near_l.at[q - 2], rs_send, rs_recv.at[2], y_at(1))

    def early_left(q):
        return remote(kept.at[q, pl.ds(0, PIECE)], near_r.at[q - 2], rs_send, rs_recv.at[2], y_at(3))

    def far_left(q):
        return remote(kept.at[q, pl.ds(0, PIECE)], far_r.at[q - 6], rs_send, rs_recv.at[q - 6], y_at(3))

    def far_right(q):
        return remote(kept.at[q, pl.ds(PIECE, PIECE)], far_l.at[q - 6], rs_send, rs_recv.at[q - 6], y_at(1))

    def late_left(q):
        return remote(kept.at[q, pl.ds(0, PIECE)], near_r.at[q - 2], rs_send, rs_recv.at[2], y_at(3))

    def late_right(q):
        return remote(kept.at[q, pl.ds(PIECE, PIECE)], near_l.at[q - 2], rs_send, rs_recv.at[2], y_at(1))

    packed = [(*(ref.at[k] for ref in (wg, s1g, t1g, vg, s2g, t2g)), out) for k, out in enumerate((ga_out, up_out))]
    packed.append((wd, s1d, t1d, vd, s2d, t2d, dn_out))
    halves = ((x, z, x_at, z_at), (z, x, z_at, x_at))
    streams = [(h, k) for k in range(3) for h in range(2)]

    class Ring:
        def __init__(self, h, k, src, base, size, mid, end, index, at, sem):
            self.src, self.size, self.mid, self.end = src, size, mid, end
            half = size // 2
            self.half = half
            f = h * 3 + k

            def rows(chunk, part):
                start = base + ((index + chunk) % 4) * size + part * half
                return pl.ds(pl.multiple_of(start, 16), half)

            self.rows = rows

            def copy(i, chunk, part, dst, to):
                return remote(src.at[rows(chunk, part)], dst, ar_send.at[f, sem], ar_recv.at[f, 2 * sem + i], at(to))

            self.sems = ar_send.at[f, sem], ar_recv.at[f, 2 * sem], ar_recv.at[f, 2 * sem + 1]
            self.bytes = lambda n: packed[k][0].at[pl.ds(0, n)]

            self.first = [
                copy(0, 2, 0, mid.at[h, 1], 3),
                copy(0, 2, 1, mid.at[h, 0], 1),
                copy(1, 3, 1, end.at[h, 1, pl.ds(half, half)], 3),
                copy(1, 1, 0, end.at[h, 0, pl.ds(0, half)], 1),
            ]
            self.second = [
                copy(1, 3, 0, end.at[h, 1, pl.ds(0, half)], 3),
                copy(1, 1, 1, end.at[h, 0, pl.ds(half, half)], 1),
            ]
            self.h = h

        def mid_out(self):
            for c in self.first[:2]:
                c.start()

        def end_out(self):
            for c in self.first[2:]:
                c.start()

        def relay(self):
            h = self.h
            taken(self.bytes(self.size), self.sems[1])
            for i, (chunk, part, side) in enumerate(((3, 0, 1), (1, 1, 0))):
                rows = self.rows(chunk, part)
                self.src[rows, :] = (self.src[rows, :].astype(F32) + self.mid[h, side].astype(F32)).astype(BF16)
                self.second[i].start()

        def finish(self, store):
            h = self.h
            taken(self.bytes(2 * self.size), self.sems[2])
            for part in range(2):
                local = pl.ds(part * self.half, self.half)
                total = self.src[self.rows(0, part), :].astype(F32)
                total = total + self.end[h, 0, local, :].astype(F32) + self.end[h, 1, local, :].astype(F32)
                store(part, total.astype(BF16))

        def drain(self):
            taken(self.bytes(3 * self.size), self.sems[0])

    rings1, rings2 = {}, {}
    for h, k in streams:
        w, s1, t1, v, s2, t2, out = packed[k]
        i1, i2, at1, at2 = halves[h]
        unit = UNITS[k]
        rings1[h, k] = Ring(h, k, w, h * 16 * unit, 4 * unit, s1, t1, i1, at1, 0)
        rings2[h, k] = Ring(h, k, v, h * 4 * unit, unit, s2, t2, i2, at2, 1)

    def step(s, carry):
        with scope("w_sib"):

            @pl.when(s < STEPS - 1)
            def _():
                to_sib(s).wait_recv()

            @pl.when(s == STEPS - 1)
            def _():
                last_in(0)

        with scope("pre"):
            pre[:, :FF] = dot(xg[s, 0], wg[0], 1, 0)
            pre[:, FF:] = dot(xg[s, 0], wg[1], 1, 0)

        def gates(r):
            rows = pl.ds(r, 32)
            gate_pre, up_pre = pre[rows, :FF], pre[rows, FF:]
            grad_hidden = 0.5 * gh[rows, :]
            sigma = jax.nn.sigmoid(gate_pre)
            active = gate_pre * sigma
            hid[rows, :] = (active * up_pre).astype(BF16)
            dgu[rows, :FF] = (grad_hidden * up_pre * sigma * (1.0 + gate_pre * (1.0 - sigma))).astype(BF16)
            dgu[rows, FF:] = (grad_hidden * active).astype(BF16)

        def hidden_grads(low):
            rows = pl.ds(low, HALF)
            gh[rows, :] = dot(xg[s, 1, rows, :], wdn[...], 1, 1)
            over(HALF, 32, lambda r: gates(low + r))

        @pl.when(s == STEPS - 1)
        def _():
            with scope("w_last"):
                last_pass(1)
                last_pass(2)

        with scope("gh"):
            hidden_grads(0)

        @pl.when(s == STEPS - 1)
        def _():
            with scope("w_last"):
                last_in(1)
                last_in(2)

        with scope("gh"):
            hidden_grads(HALF)

        def part_gu(c, width):
            cols = pl.ds(pl.multiple_of(c, width), width)
            return cols, acc_gu[cols, :] + dot(xg[s, 0, :, cols], dgu[...], 0, 0)

        def part_dn(c, store):
            value = dot(hid[...], xg[s, 1, :, pl.ds(c, WIDE)], 0, 0)
            for i in range(WIDE // CH):
                rows = pl.ds(pl.multiple_of((c // CH + i) * FF, FF), FF)
                store(rows, acc_dn[rows, :] + value[:, i * CH : (i + 1) * CH])

        @pl.when(s < STEPS - 1)
        def _():
            def keep_dn(rows, value):
                acc_dn[rows, :] = value

            def weights(c):
                cols, value = part_gu(c, WIDE)
                acc_gu[cols, :] = value
                part_dn(c, keep_dn)

            with scope("weights"):
                over(D, WIDE, weights)

        @pl.when(s == STEPS - 1)
        def _():
            def last_gu(c):
                cols, value = part_gu(c, CH)
                wg[0, cols, :] = value[:, :FF].astype(BF16)
                wg[1, cols, :] = value[:, FF:].astype(BF16)

            def last_dn(rows, value):
                wd[rows, :] = value.astype(BF16)

            for n in (2, 3, 1, 0):
                with scope("last_gu"):
                    for h in range(2):
                        last_gu((h * 4 + (halves[h][0] + n) % 4) * CH)
                for h in range(2):
                    if n == 2:
                        rings1[h, 0].mid_out()
                    if n == 1:
                        rings1[h, 0].end_out()
                        rings1[h, 1].mid_out()
            with scope("last_dn"):
                over(D, WIDE, lambda c: part_dn(c, last_dn))

        @pl.when((s >= 1) & (s < STEPS - 2))
        def _():
            with scope("w_nbr"):
                arrival(s + 1)
            to_sib(s + 1).start()

        @pl.when(s == STEPS - 2)
        def _():
            with scope("w_nbr"):
                last_pass(0)

        @pl.when(s == 1)
        def _():
            onward(s + 1, 0).start()

        @pl.when(s == 3)
        def _():
            onward(s + 1, 1).start()

        @pl.when(s == 2)
        def _():
            for q in range(3):
                last_onward(0, q).start()

        @pl.when(s == 4)
        def _():
            for q in range(3):
                last_onward(1, q).start()

        @pl.when(s >= 2)
        def _():
            sib_sum(s).wait_send()

        def terms(c):
            cols = pl.ds(c, WIDE)
            term = dot(dgu[...], wgu_t[:, cols], 1, 0).astype(BF16)
            kept[s, :, cols] = term[:HALF]
            away[s % 2, :, cols] = term[HALF:]

        with scope("terms"):
            over(D, WIDE, terms)

        @pl.when(s >= 1)
        def _():
            with scope("chipsum"):
                chip_sum(s - 1)

        sib_sum(s).start()

        @pl.when((s == 3) | (s == 4))
        def _():
            early_right(s - 1).start()

        @pl.when((s == 5) | (s == 6))
        def _():
            early_left(s - 1).start()

        return carry

    lax.fori_loop(0, STEPS, step, 0)

    def add_far(q, lo, far):
        def add(r):
            rows = pl.ds(lo + r, 32)
            kept[q, rows, :] = (kept[q, rows, :].astype(F32) + far[pl.ds(r, 32), :].astype(F32)).astype(BF16)

        over(PIECE, 32, add)

    def store_v(h, k):
        v, unit = packed[k][3], UNITS[k]

        def store(part, value):
            v[pl.ds(h * 4 * unit + part * 2 * unit, 2 * unit), :] = value

        return store

    class Back:
        def __init__(self, h, k):
            i1, i2, at1, at2 = halves[h]
            out, f, unit = packed[k][6], h * 3 + k, UNITS[k]
            half = unit // 2

            def spot(ra, rb, part=None):
                a, b = (i1 + ra) % 4, (i2 + rb) % 4
                rows = half if part is not None else unit
                if k < 2:
                    start = ((h * 4 + a) * 4 + b) * unit + (part or 0) * half
                    return pl.ds(pl.multiple_of(start, 16), rows), slice(None)
                start = b * unit + (part or 0) * half
                return pl.ds(pl.multiple_of(start, 16), rows), pl.ds(pl.multiple_of((h * 4 + a) * CH, CH), CH)

            def copy(i, to, *where):
                view = out.at[spot(*where)]
                return remote(view, view, ar_send.at[f, 2], ar_recv.at[f, 4 + i], to)

            self.taken = lambda units, sem: taken(packed[k][0].at[pl.ds(0, units * unit)], sem)
            self.sems = ar_send.at[f, 2], [ar_recv.at[f, 4 + i] for i in range(6)]

            self.out, self.spot = out, spot
            self.own2 = [copy(0, at2(1), 0, 0), copy(0, at2(3), 0, 0)]
            self.on2 = [copy(1, at2(1), 0, 3, 0), copy(1, at2(3), 0, 1, 1)]
            rightward, leftward = (2, 5, 5, 3), (5, 3, 4, 5)
            self.out1 = [
                [copy(rightward[r], at1(1), 0, r), copy(leftward[r], at1(3), 0, r)] for r in range(4)
            ]
            self.on1 = {
                0: copy(5, at1(1), 3, 0),
                3: copy(5, at1(1), 3, 3),
                1: copy(5, at1(3), 1, 1),
                2: copy(5, at1(3), 1, 2),
            }

        def store(self, part, value):
            self.out[self.spot(0, 0, part)] = value

        def send(self, r):
            for c in self.out1[r]:
                c.start()

        def begin(self):
            for c in self.own2:
                c.start()
            self.send(0)

        def middle(self):
            self.taken(2, self.sems[1][0])
            for on, r in zip(self.on2, (3, 1)):
                on.start()
                self.send(r)

        def last(self):
            self.taken(1, self.sems[1][1])
            self.send(2)

        def pass_on(self, *which):
            self.taken(len(which), self.sems[1][{0: 2, 3: 3, 2: 4}[which[0]]])
            for r in which:
                self.on1[r].start()

        def finish(self):
            self.taken(8, self.sems[1][5])

        def drain(self):
            self.taken(15, self.sems[0])

    back = {(h, k): Back(h, k) for h, k in streams}

    def own_rows(i, carry):
        r = pl.multiple_of(i * 16, 16)
        s, p = i // 8, i // 4
        half, piece = pl.ds(pl.multiple_of((i % 8) * 16, 16), 16), pl.ds(pl.multiple_of((i % 4) * 16, 16), 16)
        grad = kept[s, half, :].astype(F32) + near_l[p, piece, :].astype(F32) + near_r[p, piece, :].astype(F32)
        floats = away[s, half, :].astype(F32)
        inverse = lax.rsqrt(jnp.mean(floats * floats, axis=-1, keepdims=True) + norm_eps)
        unit_rows = floats * inverse
        gained = grad * unit_rows
        g_acc[...] += gained[:8] + gained[8:]
        scaled = grad * gain[...]
        mean = jnp.mean(scaled * unit_rows, axis=-1, keepdims=True)
        result = xg[s, 1, half, :].astype(F32) + inverse * scaled - unit_rows * inverse * mean
        gin_out[pl.ds(r, 16), :] = result.astype(BF16)
        return carry


    def spread(buffer, index, targets, group):
        for to in targets:
            remote(buffer.at[index], buffer.at[index], gn_send.at[group], gn_recv.at[group], to).start()

    def gathered(buffer, count, group):
        for sems in (gn_recv, gn_send):
            taken(buffer.at[pl.ds(0, count)], sems.at[group])

    def both(k, act):
        for h in range(2):
            act(h, k)

    def relay1(h, k):
        rings1[h, k].relay()

    def finish1(h, k):
        rings1[h, k].finish(store_v(h, k))
        rings2[h, k].mid_out()
        rings2[h, k].end_out()

    def relay2(h, k):
        rings2[h, k].relay()

    def finish2(h, k):
        rings2[h, k].finish(back[h, k].store)
        back[h, k].begin()

    def near2(h, k):
        back[h, k].middle()

    def far2(h, k):
        back[h, k].last()

    def pass0(h, k):
        back[h, k].pass_on(0)

    def pass1(h, k):
        back[h, k].pass_on(3, 1)

    def pass2(h, k):
        back[h, k].pass_on(2)

    def far1(h, k):
        back[h, k].finish()

    def run(name, k, act):
        with scope(f"{name}{k}"):
            both(k, act)

    far_left(6).start()
    far_right(6).start()

    def far(i):
        with scope("far"):
            taken(kept.at[0], rs_recv.at[i])
            add_far(2 + i, 0, far_r.at[i])
            late_left(2 + i).start()
            add_far(4 + i, PIECE, far_l.at[i])
            late_right(4 + i).start()

    def drain_gather():
        taken(xg.at[pl.ds(0, 7)], ag_send)

    def drain_tokens():
        taken(kept.at[pl.ds(0, 6)], rs_send)

    def drain_rings(rings, k):
        both(k, lambda h, k: rings[h, k].drain())

    def drain_out(k):
        both(k, lambda h, k: back[h, k].drain())

    run("relay1", 0, relay1)
    both(2, lambda h, k: rings1[h, k].mid_out())
    with scope("chip7"):
        chip_sum(7)
    far_left(7).start()
    far_right(7).start()
    run("relay1", 1, relay1)
    sib_sum(6).wait_send()
    sib_sum(7).wait_send()
    again = [pltpu.make_async_copy(x_in.at[pl.ds(s * HALF, HALF)], away.at[s], ld_sem.at[s]) for s in range(2)]
    for c in again:
        c.start()
    run("finish1", 0, finish1)
    both(1, lambda h, k: rings1[h, k].end_out())
    run("relay1", 2, relay1)
    drain_gather()
    run("relay2", 0, relay2)
    both(2, lambda h, k: rings1[h, k].end_out())
    far(0)
    run("finish1", 1, finish1)
    drain_rings(rings1, 0)
    drain_rings(rings1, 1)
    run("finish2", 0, finish2)
    run("finish1", 2, finish1)
    far(1)
    run("relay2", 1, relay2)
    run("near2", 0, near2)
    run("relay2", 2, relay2)
    run("finish2", 1, finish2)
    run("far2", 0, far2)
    run("pass1", 0, pass1)
    run("finish2", 2, finish2)
    with scope("w_rs"):
        for c in again:
            c.wait()
        taken(kept.at[pl.ds(0, 4)], rs_recv.at[2])
    with scope("own"):
        g_acc[...] = jnp.zeros((8, D), F32)
        lax.fori_loop(0, ROWS // 16, own_rows, 0, unroll=2)
        g_tp[tp] = jnp.sum(g_acc[...], axis=0, keepdims=True)
    spread(g_tp, tp, [sib], 0)
    run("near2", 1, near2)
    drain_rings(rings1, 2)
    drain_tokens()
    run("near2", 2, near2)
    with scope("g1"):
        gathered(g_tp, 1, 0)
        g_y[fs] = g_tp[0] + g_tp[1]
        spread(g_y, fs, [y_at(1), y_at(2), y_at(3)], 1)
    run("pass2", 0, pass2)
    run("pass0", 1, pass0)
    drain_rings(rings2, 0)
    run("far2", 1, far2)
    drain_rings(rings2, 1)
    drain_rings(rings2, 2)
    run("far2", 2, far2)
    with scope("g2"):
        gathered(g_y, 3, 1)
        g_rep[rep] = (g_y[0] + g_y[1]) + (g_y[2] + g_y[3])
        spread(g_rep, rep, plane, 2)
    run("pass1", 1, pass1)
    run("pass1", 2, pass1)
    run("pass2", 1, pass2)
    run("pass0", 2, pass0)
    run("pass0", 0, pass0)
    run("pass2", 2, pass2)
    with scope("g3"):
        gathered(g_rep, 15, 2)
        total = g_rep[0]
        for i in range(1, 16):
            total = total + g_rep[i]
        gain_out[...] = total
    run("far1", 0, far1)
    run("far1", 1, far1)
    run("far1", 2, far1)

    for k in range(3):
        drain_out(k)


def fused(tokens_in, norm_gain, gate_weight, up_weight, down_weight, out_grad):
    any_space = pl.BlockSpec(memory_space=pl.ANY)
    vmem = pl.BlockSpec(memory_space=pltpu.VMEM)
    (ug, _, ud), (cg, _, cd) = UNITS, WIDTHS
    dma = pltpu.SemaphoreType.DMA
    scratch = [
        pltpu.VMEM((STEPS, 2, ROWS, D), BF16),
        pltpu.VMEM((2, D, FF), BF16),
        pltpu.VMEM((FF, D), BF16),
        pltpu.VMEM((2 * FF, D), BF16),
        pltpu.VMEM((1, D), F32),
        pltpu.VMEM((D, 2 * FF), F32),
        pltpu.VMEM((8 * FF, CH), F32),
        pltpu.VMEM((ROWS, 2 * FF), F32),
        pltpu.VMEM((ROWS, FF), F32),
        pltpu.VMEM((ROWS, 2 * FF), BF16),
        pltpu.VMEM((ROWS, FF), BF16),
        pltpu.VMEM((STEPS, HALF, D), BF16),
        pltpu.VMEM((2, HALF, D), BF16),
        pltpu.VMEM((STEPS, HALF, D), BF16),
        pltpu.VMEM((2, PIECE, D), BF16),
        pltpu.VMEM((2, PIECE, D), BF16),
        pltpu.VMEM((4, PIECE, D), BF16),
        pltpu.VMEM((4, PIECE, D), BF16),
        pltpu.VMEM((8 * FF, cd), BF16),
        pltpu.VMEM((2, 2, 2, 2 * ug, cg), BF16),
        pltpu.VMEM((2, 2, 2 * ud, cd), BF16),
        pltpu.VMEM((2, 2, 2, 4 * ug, cg), BF16),
        pltpu.VMEM((2, 2, 4 * ud, cd), BF16),
        pltpu.VMEM((2, 2 * 4 * ug, cg), BF16),
        pltpu.VMEM((2 * 4 * ud, cd), BF16),
        pltpu.VMEM((2, 2, 2, ug // 2, cg), BF16),
        pltpu.VMEM((2, 2, ud // 2, cd), BF16),
        pltpu.VMEM((2, 2, 2, ug, cg), BF16),
        pltpu.VMEM((2, 2, ud, cd), BF16),
        pltpu.VMEM((8, D), F32),
        pltpu.VMEM((2, 1, D), F32),
        pltpu.VMEM((4, 1, D), F32),
        pltpu.VMEM((16, 1, D), F32),
        dma((8,)),
        dma,
        dma((STEPS, 2)),
        dma((2, 3)),
        dma((2,)),
        dma((STEPS,)),
        dma,
        dma((3,)),
        dma((6, 3)),
        dma((6, 10)),
        dma((3,)),
        dma((3,)),
    ]
    return pl.pallas_call(
        kernel,
        name="fused",
        out_shape=(
            pltpu.VMEM((ROWS, D), BF16),
            pltpu.VMEM((1, D), F32),
            pltpu.VMEM((D, FF), BF16),
            pltpu.VMEM((D, FF), BF16),
            pltpu.VMEM((FF, D), BF16),
        ),
        in_specs=[any_space] * 6,
        out_specs=(vmem,) * 5,
        scratch_shapes=scratch,
        compiler_params=pltpu.CompilerParams(
            collective_id=0, has_side_effects=True, vmem_limit_bytes=60_800_000
        ),
    )(tokens_in, norm_gain.reshape(1, D), gate_weight, up_weight, down_weight, out_grad)


def scaled(factor, ga, up, dn, gin, gain, ga_out, up_out, dn_out, gin_out, gain_out, fa, fu, fd, sems):
    copies = [
        pltpu.make_async_copy(gin, gin_out, sems.at[0]),
        pltpu.make_async_copy(gain, gain_out, sems.at[1]),
    ]
    for c in copies:
        c.start()

    def piece(i, src, mid, out, start, size, step, scale):
        def convert(r):
            rows = pl.ds(start + r, step)
            mid[rows, :] = src[rows, :].astype(F32) * scale

        over(size, step, convert)
        rows = pl.ds(start, size)
        copies.append(pltpu.make_async_copy(mid.at[rows], out.at[rows], sems.at[i]))
        copies[-1].start()

    for n in range(8):
        piece(2 + n, ga, fa, ga_out, n * 256, 256, 64, factor)
        piece(10 + n, up, fu, up_out, n * 256, 256, 64, factor)
    for n in range(8):
        piece(18 + n, dn, fd, dn_out, n * 48, 48, 16, 0.5 * factor)
    for c in copies:
        c.wait()


def shards(tokens_in, norm_gain, gate_weight, up_weight, down_weight, out_grad):
    row_count = tokens_in.shape[0]
    total_tokens = row_count * lax.axis_size("rep") * lax.axis_size("fs") * lax.axis_size("tp")
    factor = float(total_tokens) ** (-0.5)
    grad_in, gain_row, ga, up, dn = fused(tokens_in, norm_gain, gate_weight, up_weight, down_weight, out_grad)
    shapes = ((D, FF), (D, FF), (FF, D))
    grad_gate, grad_up, grad_down, grad_in, gain_row = pl.pallas_call(
        functools.partial(scaled, factor),
        name="scaled",
        out_shape=(
            *(jax.ShapeDtypeStruct(shape, F32) for shape in shapes),
            jax.ShapeDtypeStruct((ROWS, D), BF16),
            jax.ShapeDtypeStruct((1, D), F32),
        ),
        in_specs=[pl.BlockSpec(memory_space=pltpu.VMEM)] * 5,
        out_specs=(pl.BlockSpec(memory_space=pl.ANY),) * 5,
        scratch_shapes=[*(pltpu.VMEM(shape, F32) for shape in shapes), pltpu.SemaphoreType.DMA((26,))],
        compiler_params=pltpu.CompilerParams(vmem_limit_bytes=30_000_000),
    )(*(pltpu.with_memory_space_constraint(v, pltpu.VMEM) for v in (ga, up, dn, grad_in, gain_row)))
    grad_gain = gain_row.reshape(D)
    return (grad_in, grad_gain, grad_gate, grad_up, grad_down)


def solution(mesh):
    in_specs = (
        P(("rep", "fs", "tp"), None),
        P(),
        P(None, ("fs", "tp")),
        P(None, ("fs", "tp")),
        P(("fs", "tp"), None),
        P(("rep", "fs", "tp"), None),
    )
    out_specs = (
        P(("rep", "fs", "tp"), None),
        P(),
        P(None, ("fs", "tp")),
        P(None, ("fs", "tp")),
        P(("fs", "tp"), None),
    )
    return jax.shard_map(shards, mesh=mesh, in_specs=in_specs, out_specs=out_specs, check_vma=False)
```
